32 devices in a mesh: sp: 8 (over z, x), tp: 4 (over y, core).
Axes of the slice: x: 2, y: 2, z: 4, core: 2. Of those that a mesh axis runs over, the one named last changes fastest.
Arguments:
- tokens: bfloat16 [1024, 2048], P(('sp', 'tp')), may hold values from -6 to 6
- input_norm_gain: float32 [2048], replicated, may hold values from 0.1 to 1.9
- convolution_value_weight: bfloat16 [2048, 1024], P('sp', 'tp'), may hold values from -0.125 to 0.125
- convolution_gate_weight: bfloat16 [2048, 1024], P('sp', 'tp'), may hold values from -0.125 to 0.125
- depthwise_filter_taps: float32 [31, 1024], P(None, 'tp'), may hold values from -4 to 4
- channel_norm_gain: float32 [1024], P('tp'), may hold values from 0.1 to 1.9
- channel_norm_bias: float32 [1024], P('tp'), may hold values from -3 to 3
- query_projection_weight: bfloat16 [2048, 1024], P('sp', 'tp'), may hold values from -0.125 to 0.125
- forget_gate_weight: bfloat16 [2048, 1024], P('sp', 'tp'), may hold values from -0.125 to 0.125
- recurrence_value_weight: bfloat16 [2048, 1024], P('sp', 'tp'), may hold values from -0.125 to 0.125
- output_gate_weight: bfloat16 [2048, 1024], P('sp', 'tp'), may hold values from -0.125 to 0.125
- forget_floor_margin: float32 [1024], P('tp'), may hold values from 9.765625e-05 to 0.1
- decay_jump_terms: float32 [8, 1024], P('tp', 'sp'), may hold values from -0.7 to 0
- head_norm_gain: float32 [1024], P('tp'), may hold values from 0.1 to 1.9
- convolution_output_weight: bfloat16 [1024, 2048], P('tp', 'sp'), may hold values from -0.125 to 0.125
- recurrence_output_weight: bfloat16 [1024, 2048], P('tp', 'sp'), may hold values from -0.125 to 0.125
Outputs:
- mixed: bfloat16 [1024, 2048], P(('sp', 'tp'))
The draws below stay inside these ranges and needn't reach their ends.
All inputs are finite; a program needn't handle non-finite values.
Results may differ from the reference program's by a relative error of at most 0.015.
Values may be sent and summed in bfloat16 or wider, within the bound.
A program may use at most 64 MiB of HBM per device.

```python
import math
import jax
import jax.numpy as jnp
from jax import lax

D = 2048
CONV_CH = 1024
CONV_W = 31
HG_HEADS = 8
HG_DK = 128
HG_DV = 128
HG_BLOCK = 64
TOK_DEV = 128
TOKENS = 1024
N_TP = 4


def draw_depthwise_filter_taps(key, part):
    noise_key, scale_key = jax.random.split(key, 2)
    channel = jnp.arange(CONV_CH, dtype=jnp.float32) / CONV_CH
    jitter = jax.random.uniform(scale_key, (CONV_CH,), jnp.float32, -1.15, 1.15)
    scales = jnp.exp(math.log(3.0) * channel + jitter) / 3.0
    noise_draw = jax.random.normal(noise_key, (CONV_W, CONV_CH), jnp.float32)
    return jnp.clip(noise_draw * scales / math.sqrt(CONV_W), -4.0, 4.0)


def draw_forget_floor_margin(key, part):
    order_key, slow_key, fast_key = jax.random.split(key, 3)
    order = jax.random.permutation(order_key, HG_HEADS)
    slow_head = jnp.repeat(order < HG_HEADS // 2, HG_DK)
    slow_gap = jnp.exp(jax.random.uniform(slow_key, (HG_HEADS * HG_DK,), jnp.float32, math.log(0.1), math.log(0.5))) / TOKENS
    fast_gap = jnp.exp(jax.random.uniform(fast_key, (HG_HEADS * HG_DK,), jnp.float32, math.log(0.03), math.log(0.1)))
    return jnp.where(slow_head, slow_gap, fast_gap)


def draw_decay_jump_terms(key, part):
    rate_key, place_key, depth_key = jax.random.split(key, 3)
    block_total = TOKENS // TOK_DEV
    third = TOKENS // 3
    rates = jnp.exp(jax.random.uniform(rate_key, (HG_HEADS, block_total), jnp.float32, math.log(0.15), math.log(0.6))) / TOKENS
    decay_depths = jnp.log(jax.random.uniform(depth_key, (HG_HEADS, 2), jnp.float32, 0.55, 0.8))
    place_indices = jax.random.randint(place_key, (HG_HEADS, 2), 0, third) + jnp.arange(2)[None, :] * third
    steady_decay = -jnp.repeat(rates, TOK_DEV, axis=1)
    position_indices = jnp.arange(TOKENS)
    decay_jumps = jnp.sum(jnp.where(position_indices[None, None, :] == place_indices[:, :, None], decay_depths[:, :, None], 0.0), axis=1)
    return steady_decay + decay_jumps


def shard_levels(stream_key, extent, cuts, low, high):
    level, own = 1.0, jax.random.fold_in(stream_key, 6)
    for axis_at, shards_of in cuts:
        draws = jnp.exp(jax.random.uniform(jax.random.fold_in(own, axis_at), (shards_of,), jnp.float32, low / len(cuts), high / len(cuts)))
        level = level * jnp.repeat(draws, extent[axis_at] // shards_of).reshape([-1 if axis == axis_at else 1 for axis in range(len(extent))])
    return level


def scatter_about(rng, extent, scale, bound, cuts=(), held_as=jnp.bfloat16):
    loudness = shard_levels(rng, extent, cuts, -0.22, 0.18) if cuts else 1.0
    entries = jax.random.normal(rng, extent, jnp.float32) * scale * loudness
    return jnp.minimum(jnp.maximum(entries, -bound), bound).astype(held_as)


def setup_inputs(seed: int = 0) -> dict:
    splits = jax.random.split(jax.random.key(seed), 17)
    tokens = scatter_about(splits[0], (TOKENS, D), 1.0, 6.0, ((0, 32),))
    input_norm_gain = jnp.clip(1.0 + 0.18 * jax.random.normal(splits[1], (D,), jnp.float32), 0.1, 1.9)
    convolution_value_weight = scatter_about(splits[2], (D, CONV_CH), D ** -0.5, 0.125, ((0, 8), (1, 4)))
    convolution_gate_weight = scatter_about(splits[3], (D, CONV_CH), D ** -0.5, 0.125, ((0, 8), (1, 4)))
    depthwise_filter_taps = draw_depthwise_filter_taps(jax.random.fold_in(splits[16], 71), 0)
    channel_norm_gain = jnp.clip(1.0 + 0.18 * jax.random.normal(splits[5], (CONV_CH,), jnp.float32), 0.1, 1.9)
    channel_norm_bias = scatter_about(splits[6], (CONV_CH,), 0.5, 3.0, ((0, 4),), jnp.float32)
    query_projection_weight = scatter_about(splits[7], (D, HG_HEADS * HG_DK), D ** -0.5, 0.125, ((0, 8), (1, 4)))
    forget_gate_weight = scatter_about(splits[8], (D, HG_HEADS * HG_DK), D ** -0.5, 0.125, ((0, 8), (1, 4)))
    recurrence_value_weight = scatter_about(splits[9], (D, HG_HEADS * HG_DV), D ** -0.5, 0.125, ((0, 8), (1, 4)))
    output_gate_weight = scatter_about(splits[10], (D, HG_HEADS * HG_DV), D ** -0.5, 0.125, ((0, 8), (1, 4)))
    forget_floor_margin = draw_forget_floor_margin(jax.random.fold_in(splits[16], 71), 0)
    decay_jump_terms = draw_decay_jump_terms(jax.random.fold_in(splits[16], 71), 0)
    head_norm_gain = jnp.clip(1.0 + 0.18 * jax.random.normal(splits[13], (HG_HEADS * HG_DV,), jnp.float32), 0.1, 1.9)
    convolution_output_weight = scatter_about(splits[14], (CONV_CH, D), (CONV_CH + HG_HEADS * HG_DV) ** -0.5, 0.125, ((0, 4), (1, 8)))
    recurrence_output_weight = scatter_about(splits[15], (HG_HEADS * HG_DV, D), (CONV_CH + HG_HEADS * HG_DV) ** -0.5, 0.125, ((0, 4), (1, 8)))
    return {"tokens": tokens, "input_norm_gain": input_norm_gain, "convolution_value_weight": convolution_value_weight, "convolution_gate_weight": convolution_gate_weight, "depthwise_filter_taps": depthwise_filter_taps, "channel_norm_gain": channel_norm_gain, "channel_norm_bias": channel_norm_bias, "query_projection_weight": query_projection_weight, "forget_gate_weight": forget_gate_weight, "recurrence_value_weight": recurrence_value_weight, "output_gate_weight": output_gate_weight, "forget_floor_margin": forget_floor_margin, "decay_jump_terms": decay_jump_terms, "head_norm_gain": head_norm_gain, "convolution_output_weight": convolution_output_weight, "recurrence_output_weight": recurrence_output_weight}


norm_eps = 1e-06
layer_eps = 1e-05
highest_precision = lax.Precision.HIGHEST

def convolve(gated, kernel):
    return lax.conv_general_dilated(gated[None], kernel[:, None, :], (1,), 'VALID', dimension_numbers=('NWC', 'WIO', 'NWC'), feature_group_count=gated.shape[1], precision=highest_precision)[0]

def channel_norm(values, first_sum, second_sum, gain, bias):
    mean_value = first_sum[:, None] / CONV_CH
    variance = second_sum[:, None] / CONV_CH - mean_value * mean_value
    shifted = (values - mean_value) * lax.rsqrt(variance + layer_eps) * gain + bias
    return jax.nn.silu(shifted).astype(jnp.bfloat16)

def gate_factors(query_projected, forget_projected, forget_floor_margin, decay_jump_rows):
    row_total_count = query_projected.shape[0]
    head_total_count = decay_jump_rows.shape[1]
    query_rows = jax.nn.silu(query_projected.astype(jnp.float32))
    log_forget_gate = jnp.logaddexp(jnp.log1p(-forget_floor_margin), jnp.log(forget_floor_margin) + jax.nn.log_sigmoid(forget_projected.astype(jnp.float32)))
    key_gate_values = -jnp.expm1(log_forget_gate)
    log_decay_running = log_forget_gate.reshape(row_total_count, head_total_count, -1) + decay_jump_rows[:, :, None]
    return (query_rows.reshape(row_total_count, head_total_count, -1), key_gate_values.reshape(row_total_count, head_total_count, -1), log_decay_running)

def finish(recurrent, gain, outgate_proj):
    row_total_count = recurrent.shape[0]
    scaled = recurrent * lax.rsqrt(lax.optimization_barrier(jnp.mean(recurrent * recurrent, axis=2, keepdims=True)) + norm_eps)
    gated_out = scaled.reshape(row_total_count, -1) * gain * jax.nn.silu(outgate_proj.astype(jnp.float32))
    return gated_out.astype(jnp.bfloat16)

def block_step(recurrence_state, block_parts):
    query_rows, key_gate_values, input_rows, log_decay_running = block_parts
    block_len = query_rows.shape[1]
    cumulative = jnp.cumsum(log_decay_running, axis=1)
    final_decay = cumulative[:, -1:, :]
    query_rows_scaled = query_rows * jnp.exp(cumulative)
    scaled_keys = key_gate_values * jnp.exp(-cumulative)
    final_keys = key_gate_values * jnp.exp(final_decay - cumulative)
    attention_scores = jnp.einsum('htk,hsk->hts', query_rows_scaled, scaled_keys, precision=highest_precision)
    causal = jnp.arange(block_len)[:, None] >= jnp.arange(block_len)[None, :]
    attention_scores = jnp.where(causal[None], attention_scores, 0.0)
    output_rows = jnp.einsum('mby,myx->mbx', attention_scores, input_rows, precision=highest_precision) + jnp.einsum('ufi,uij->ufj', query_rows_scaled, recurrence_state, precision=highest_precision)
    recurrence_state = jnp.exp(final_decay[:, 0, :])[:, :, None] * recurrence_state + jnp.einsum('meg,met->mgt', final_keys, input_rows, precision=highest_precision)
    return (recurrence_state, output_rows)

def reference(tokens, input_norm_gain, convolution_value_weight, convolution_gate_weight, depthwise_filter_taps, channel_norm_gain, channel_norm_bias, query_projection_weight, forget_gate_weight, recurrence_value_weight, output_gate_weight, forget_floor_margin, decay_jump_terms, head_norm_gain, convolution_output_weight, recurrence_output_weight):
    features = tokens.astype(jnp.float32)
    normed = (features * lax.rsqrt(lax.optimization_barrier(jnp.mean(features * features, axis=1, keepdims=True)) + norm_eps) * input_norm_gain).astype(jnp.bfloat16)

    def project(weight):
        return jnp.dot(normed, weight, preferred_element_type=jnp.float32).astype(jnp.bfloat16)
    value_proj = project(convolution_value_weight)
    gate_proj = project(convolution_gate_weight)
    query_projected = project(query_projection_weight)
    forget_projected = project(forget_gate_weight)
    input_proj = project(recurrence_value_weight)
    outgate_proj = project(output_gate_weight)
    gated = value_proj.astype(jnp.float32) * jax.nn.sigmoid(gate_proj.astype(jnp.float32))
    padded = jnp.pad(gated, ((CONV_W - 1, 0), (0, 0)))
    convolved = convolve(padded, depthwise_filter_taps).astype(jnp.bfloat16)
    values = convolved.astype(jnp.float32)
    conv_out = channel_norm(values, lax.optimization_barrier(jnp.sum(values, axis=1)), lax.optimization_barrier(jnp.sum(values * values, axis=1)), channel_norm_gain, channel_norm_bias)
    query_rows, key_gate_values, log_decay_running = gate_factors(query_projected, forget_projected, forget_floor_margin, decay_jump_terms.T)
    input_rows = input_proj.astype(jnp.float32).reshape(TOKENS, HG_HEADS, HG_DV)
    block_count = TOKENS // HG_BLOCK

    def to_blocks(array):
        return array.reshape(block_count, HG_BLOCK, HG_HEADS, -1).transpose(0, 2, 1, 3)
    initial = jnp.zeros((HG_HEADS, HG_DK, HG_DV), jnp.float32)
    scanned = lax.scan(block_step, initial, (to_blocks(query_rows), to_blocks(key_gate_values), to_blocks(input_rows), to_blocks(log_decay_running)))
    recurrent = scanned[1].transpose(0, 2, 1, 3).reshape(TOKENS, HG_HEADS, HG_DV)
    rec_out = finish(recurrent, head_norm_gain, outgate_proj)
    conv_group = CONV_CH // N_TP
    rec_group = HG_HEADS * HG_DV // N_TP
    summed = jnp.zeros((TOKENS, D), jnp.float32)
    for group in range(N_TP):
        conv_slice = slice(group * conv_group, (group + 1) * conv_group)
        rec_slice = slice(group * rec_group, (group + 1) * rec_group)
        partial_sum = jnp.dot(conv_out[:, conv_slice], convolution_output_weight[conv_slice], preferred_element_type=jnp.float32) + jnp.dot(rec_out[:, rec_slice], recurrence_output_weight[rec_slice], preferred_element_type=jnp.float32)
        summed = summed + lax.optimization_barrier(partial_sum.astype(jnp.bfloat16)).astype(jnp.float32)
    return summed.astype(jnp.bfloat16)
```

```python
import functools

import jax
import jax.numpy as jnp
from jax import lax
from jax.experimental import pallas as pl
from jax.experimental.pallas import tpu as pltpu
from jax.sharding import PartitionSpec as P

CONV_CH = 1024
HG_DK = 128
HG_DV = 128
HG_BLOCK = 64


norm_eps = 1e-06
layer_eps = 1e-05
highest_precision = lax.Precision.HIGHEST


def passed_along(value, axis, steps):
    count = lax.axis_size(axis)
    initial, last = (max(0, -steps), min(count, count - steps))
    return lax.ppermute(value, axis, [(source, source + steps) for source in range(initial, last)])


def prefix(x, axis, combine, identity):
    size, mine = (lax.axis_size(axis), lax.axis_index(axis))
    everything = jax.tree.map(
        lambda part, kind: lax.all_gather(part.astype(kind), axis), x, (jnp.bfloat16, jnp.bfloat16)
    )
    start = jax.tree.map(
        lambda part, zero: jnp.broadcast_to(jnp.asarray(zero, part.dtype), part.shape), x, identity
    )

    def lap(k, before):
        reached = k < mine
        new = combine(
            before, jax.tree.map(lambda part, own: part[k].astype(own.dtype), everything, x)
        )
        return jax.tree.map(lambda a, b: jnp.where(reached, a, b), new, before)

    return lax.fori_loop(0, size, lap, start)


def convolve(gated, kernel):
    return lax.conv_general_dilated(
        gated[None],
        kernel[:, None, :],
        (1,),
        "VALID",
        dimension_numbers=("NWC", "WIO", "NWC"),
        feature_group_count=gated.shape[1],
        precision=highest_precision,
    )[0]


def channel_norm(values, first_sum, second_sum, gain, bias):
    mean_value = first_sum[:, None] / CONV_CH
    variance = second_sum[:, None] / CONV_CH - mean_value * mean_value
    shifted = (values - mean_value) * lax.rsqrt(variance + layer_eps) * gain + bias
    return jax.nn.silu(shifted).astype(jnp.bfloat16)


def gate_factors(query_projected, forget_projected, forget_floor_margin, decay_jump_rows):
    row_total_count = query_projected.shape[0]
    head_total_count = decay_jump_rows.shape[1]
    query_rows = jax.nn.silu(query_projected.astype(jnp.float32))
    log_forget_gate = jnp.logaddexp(
        jnp.log1p(-forget_floor_margin),
        jnp.log(forget_floor_margin) + jax.nn.log_sigmoid(forget_projected.astype(jnp.float32)),
    )
    key_gate_values = -jnp.expm1(log_forget_gate)
    log_decay_running = (
        log_forget_gate.reshape(row_total_count, head_total_count, -1) + decay_jump_rows[:, :, None]
    )
    return (
        query_rows.reshape(row_total_count, head_total_count, -1),
        key_gate_values.reshape(row_total_count, head_total_count, -1),
        log_decay_running,
    )


def finish(recurrent, gain, outgate_proj):
    row_total_count = recurrent.shape[0]
    scaled = recurrent * lax.rsqrt(
        jnp.mean(recurrent * recurrent, axis=2, keepdims=True) + norm_eps
    )
    gated_out = (
        scaled.reshape(row_total_count, -1) * gain * jax.nn.silu(outgate_proj.astype(jnp.float32))
    )
    return gated_out.astype(jnp.bfloat16)


def combine_states(first_part, second_part):
    return (
        first_part[0] + second_part[0],
        jnp.exp(second_part[0])[:, :, None] * first_part[1] + second_part[1],
    )


def carry_step(recurrence_state, block_parts):
    decay_end, contribution = block_parts
    return (jnp.exp(decay_end)[:, :, None] * recurrence_state + contribution, recurrence_state)


def per_device(
    tokens,
    input_norm_gain,
    convolution_value_weight,
    convolution_gate_weight,
    depthwise_filter_taps,
    channel_norm_gain,
    channel_norm_bias,
    query_projection_weight,
    forget_gate_weight,
    recurrence_value_weight,
    output_gate_weight,
    forget_floor_margin,
    decay_jump_terms,
    head_norm_gain,
    convolution_output_weight,
    recurrence_output_weight,
):
    features = tokens.astype(jnp.float32)
    normed = (
        features
        * lax.rsqrt(jnp.mean(features * features, axis=1, keepdims=True) + norm_eps)
        * input_norm_gain
    ).astype(jnp.bfloat16)
    gathered = (
        lax.all_gather(convolution_value_weight, "sp", axis=0, tiled=True),
        lax.all_gather(convolution_gate_weight, "sp", axis=0, tiled=True),
        lax.all_gather(query_projection_weight, "sp", axis=0, tiled=True),
        lax.all_gather(forget_gate_weight, "sp", axis=0, tiled=True),
        lax.all_gather(recurrence_value_weight, "sp", axis=0, tiled=True),
        lax.all_gather(output_gate_weight, "sp", axis=0, tiled=True),
        lax.all_gather(convolution_output_weight, "sp", axis=1, tiled=True),
        lax.all_gather(recurrence_output_weight, "sp", axis=1, tiled=True),
    )
    projection_weights = gathered[:6]
    conv_columns = gathered[6]
    rec_columns = gathered[7]

    def project(row_piece):
        return jnp.concatenate(
            [
                jnp.dot(row_piece, weight, preferred_element_type=jnp.float32).astype(jnp.bfloat16)
                for weight in projection_weights
            ],
            axis=1,
        )

    projected = project(lax.all_gather(normed, "tp", axis=0, tiled=True))
    offsets = []
    position = 0
    for weight in projection_weights[:-1]:
        position = position + weight.shape[1]
        offsets.append(position)
    value_proj, gate_proj, query_projected, forget_projected, input_proj, outgate_proj = jnp.split(
        projected, offsets, axis=1
    )
    row_total_count = value_proj.shape[0]
    rim_rows = depthwise_filter_taps.shape[0] - 1
    tail_value, tail_gate = passed_along(
        (value_proj[row_total_count - rim_rows :], gate_proj[row_total_count - rim_rows :]), "sp", 1
    )
    value_ext = jnp.concatenate([tail_value, value_proj], axis=0)
    gate_ext = jnp.concatenate([tail_gate, gate_proj], axis=0)
    gated = value_ext.astype(jnp.float32) * jax.nn.sigmoid(gate_ext.astype(jnp.float32))
    convolved = convolve(gated, depthwise_filter_taps).astype(jnp.bfloat16)
    device_heads = decay_jump_terms.shape[0]
    query_rows, key_gate_values, log_decay_running = gate_factors(
        query_projected, forget_projected, forget_floor_margin, decay_jump_terms.T
    )
    input_rows = input_proj.astype(jnp.float32).reshape(row_total_count, device_heads, -1)
    block_count = row_total_count // HG_BLOCK

    def to_blocks(array):
        return array.reshape(block_count, HG_BLOCK, device_heads, -1).transpose(0, 2, 1, 3)

    block_queries = to_blocks(query_rows)
    block_keys = to_blocks(key_gate_values)
    block_inputs = to_blocks(input_rows)
    cumulative = jnp.cumsum(to_blocks(log_decay_running), axis=2)
    final_decay = cumulative[:, :, -1, :]
    query_rows_scaled = block_queries * jnp.exp(cumulative)
    scaled_keys = block_keys * jnp.exp(-cumulative)
    final_keys = block_keys * jnp.exp(final_decay[:, :, None, :] - cumulative)
    attention_scores = jnp.einsum(
        "nhtk,nhsk->nhts", query_rows_scaled, scaled_keys, precision=highest_precision
    )
    causal = jnp.arange(HG_BLOCK)[:, None] >= jnp.arange(HG_BLOCK)[None, :]
    attention_scores = jnp.where(causal[None, None], attention_scores, 0.0)
    inner = jnp.einsum(
        "nhts,nhsv->nhtv", attention_scores, block_inputs, precision=highest_precision
    )
    contributions = jnp.einsum(
        "nhsk,nhsv->nhkv", final_keys, block_inputs, precision=highest_precision
    )
    initial = jnp.zeros((device_heads, HG_DK, HG_DV), jnp.float32)
    local_state, block_starts = lax.scan(carry_step, initial, (final_decay, contributions))
    device_decay = jnp.sum(final_decay, axis=0)
    before_blocks = jnp.cumsum(final_decay, axis=0) - final_decay
    incoming = prefix(
        (device_decay, local_state),
        "sp",
        combine_states,
        (jnp.zeros_like(device_decay), jnp.zeros_like(local_state)),
    )
    starts = block_starts + jnp.exp(before_blocks)[:, :, :, None] * incoming[1][None]
    recurrent = inner + jnp.einsum(
        "nhtk,nhkv->nhtv", query_rows_scaled, starts, precision=highest_precision
    )
    recurrent = recurrent.transpose(0, 2, 1, 3).reshape(row_total_count, device_heads, -1)
    rec_out = finish(recurrent, head_norm_gain, outgate_proj)
    values = convolved.astype(jnp.float32)
    totals = lax.psum((jnp.sum(values, axis=1), jnp.sum(values * values, axis=1)), "tp")
    conv_out = channel_norm(values, totals[0], totals[1], channel_norm_gain, channel_norm_bias)
    conv_part = lax.slice_in_dim(
        conv_out, 0, row_total_count // lax.axis_size("tp") * lax.axis_size("tp"), axis=0
    )
    return lax.psum_scatter(
        (
            jnp.dot(conv_part, conv_columns, preferred_element_type=jnp.float32)
            + jnp.dot(rec_out, rec_columns, preferred_element_type=jnp.float32)
        ).astype(jnp.bfloat16),
        "tp",
        scatter_dimension=0,
        tiled=True,
    )


MESH = pl.DeviceIdType.MESH
STRIDE = 2
NT = (((1,), (1,)), ((), ()))
TN = (((0,), (0,)), ((), ()))


def at(sp, tp):
    return {"sp": sp, "tp": tp}


def greet(peers):
    barrier = pltpu.get_barrier_semaphore()
    for peer in peers:
        pl.semaphore_signal(barrier, inc=1, device_id=peer, device_id_type=MESH)
    pl.semaphore_wait(barrier, len(peers))


def remote(src, dst, send, recv, peer):
    return pltpu.make_async_remote_copy(
        src_ref=src, dst_ref=dst, send_sem=send, recv_sem=recv, device_id=peer, device_id_type=MESH
    )


def project_kernel(
    sizes, x_ref, w_ref, j_ref, p_ref, qf_ref, jump_ref, held, weights, *sems
):
    n_sp, n_tp, rows, depth, chans, members = sizes
    (send_z, send_x, send_y, send_c, lane, sib, send_w, recv_w, send_j, recv_j, send_q, recv_q) = sems
    s, t = lax.axis_index("sp"), lax.axis_index("tp")
    n_z = n_sp // STRIDE
    z, x = s // STRIDE, s % STRIDE
    y, c = t // 2, t % 2
    x_peer = at(z * STRIDE + (1 - x), t)
    y_peer = at(s, (1 - y) * 2 + c)
    c_peer = at(s, y * 2 + (1 - c))

    def sp_peer(k):
        return lax.rem(s + k, n_sp)

    def slot(dy, dx, dz, core):
        from_z = lax.rem(z - dz + n_z, n_z)
        from_x = (1 - x) if dx else x
        from_y = (1 - y) if dy else y
        shard = (from_z * STRIDE + from_x) * n_tp + from_y * 2 + core
        return pl.ds(pl.multiple_of(shard * rows, rows), rows)

    def number(dy, dx, dz):
        return (dy * STRIDE + dx) * n_z + dz

    greet([at(sp_peer(k), t) for k in range(1, n_sp)] + [y_peer, c_peer])
    pending = []

    def launch(copy):
        copy.start()
        pending.append(copy)

    own = slot(0, 0, 0, c)

    def pass_on(dy, dx, dz, src):
        here = slot(dy, dx, dz, c)
        at_number = number(dy, dx, dz)
        if not dy:
            if not dx:
                launch(remote(src, held.at[here], send_x.at[dz], lane.at[number(0, 1, dz)], x_peer))
            launch(remote(src, held.at[here], send_y.at[at_number], lane.at[number(1, dx, dz)], y_peer))
        launch(remote(src, held.at[here], send_c.at[at_number], sib.at[at_number], c_peer))

    for k in range(1, n_z):
        peer = at(lax.rem(z + k, n_z) * STRIDE + x, t)
        launch(remote(x_ref, held.at[own], send_z.at[k], lane.at[k], peer))
    pass_on(0, 0, 0, x_ref)
    my_columns = pl.ds(pl.multiple_of(s * depth, depth), depth)
    for k in range(1, n_sp):
        launch(remote(j_ref, jump_ref.at[s], send_j.at[k], recv_j.at[k], at(sp_peer(k), t)))
    for k in range(1, n_sp):
        launch(
            remote(w_ref.at[sp_peer(k)], weights.at[:, my_columns], send_w.at[k], recv_w.at[k], at(sp_peer(k), t))
        )
    held[own, :] = x_ref[...]
    jump_ref[s] = j_ref[...]
    weights[:, my_columns] = w_ref[s]

    def arrived(dy, dx, dz):
        here = held.at[slot(dy, dx, dz, c)]
        remote(here, here, send_c.at[0], lane.at[number(dy, dx, dz)], c_peer).wait_recv()
        pass_on(dy, dx, dz, here)

    for dz in range(1, n_z):
        arrived(0, 0, dz)
    for dz in range(n_z):
        arrived(0, 1, dz)
    for dx in range(STRIDE):
        for dz in range(n_z):
            arrived(1, dx, dz)
    for k in range(1, n_sp):
        source = lax.rem(s - k + n_sp, n_sp)
        there = weights.at[:, pl.ds(pl.multiple_of(source * depth, depth), depth)]
        remote(there, there, send_w.at[k], recv_w.at[k], c_peer).wait_recv()
        remote(j_ref, jump_ref.at[source], send_j.at[k], recv_j.at[k], c_peer).wait_recv()
    for dy in range(2):
        for dx in range(STRIDE):
            for dz in range(n_z):
                here = held.at[slot(dy, dx, dz, 1 - c)]
                remote(here, here, send_c.at[0], sib.at[number(dy, dx, dz)], c_peer).wait_recv()

    member = lax.rem(s, members)
    first = s - member
    total = held.shape[0]
    step = min(256, total)
    for start in range(0, total, step):
        piece = lax.dot_general(
            held[start : start + step, :], weights[...], NT, preferred_element_type=jnp.float32
        ).T.astype(jnp.bfloat16)
        p_ref[:, start : start + step] = piece[: 4 * chans]
        qf_ref[member, :, start : start + step] = piece[4 * chans :]
    for k in range(1, members):
        peer = at(first + lax.rem(member + k, members), t)
        launch(remote(qf_ref.at[member], qf_ref.at[member], send_q.at[k], recv_q.at[k], peer))
    for k in range(1, members):
        there = qf_ref.at[lax.rem(member - k + members, members)]
        remote(there, there, send_q.at[k], recv_q.at[k], c_peer).wait_recv()
    for copy in pending:
        copy.wait_send()


def mix_kernel(sizes, p_ref, qf_ref, jump_ref, par_ref, a_ref, q_s, k_s, d_s, r_s):
    n_sp, chans, members, width, block, part = sizes
    s = lax.axis_index("sp")
    total = p_ref.shape[1]
    f32, bf16 = jnp.float32, jnp.bfloat16
    mine = par_ref[pl.ds(pl.multiple_of(s * chans, chans), chans), :]
    head = s // members
    span = chans * members
    margin = par_ref[pl.ds(pl.multiple_of(head * span, span), span), width + 1 : width + 2]

    value = p_ref[0:chans, :].astype(f32)
    gate = p_ref[chans : 2 * chans, :].astype(f32)
    gated = value * jax.nn.sigmoid(gate)
    place = lax.broadcasted_iota(jnp.int32, gated.shape, 1)
    conv = gated * mine[:, width - 1 : width]
    for back in range(1, width):
        moved = jnp.where(place >= back, pltpu.roll(gated, back, 1), 0.0)
        conv = conv + moved * mine[:, width - 1 - back : width - back]
    a_ref[0:chans, :] = conv.astype(bf16)

    picked = lax.broadcasted_iota(jnp.int32, jump_ref.shape[1:], 0) == head
    for b in range(n_sp):
        lanes = slice(b * part, (b + 1) * part)
        jump = jnp.sum(jnp.where(picked, jump_ref[b], 0.0), axis=0, keepdims=True)
        both = [qf_ref[m, :, lanes].astype(f32) for m in range(members)]
        query = jnp.concatenate([v[:chans] for v in both], axis=0)
        forget = jnp.concatenate([v[chans:] for v in both], axis=0)
        key = margin * jax.nn.sigmoid(-forget)
        q_s[lanes, :] = (query * jax.nn.sigmoid(query)).T
        k_s[lanes, :] = key.T
        d_s[lanes, :] = (jnp.log1p(-key) + jump).T
    low = lax.broadcasted_iota(jnp.int32, (block, block), 0) >= lax.broadcasted_iota(
        jnp.int32, (block, block), 1
    )
    tri = low.astype(bf16)
    inputs = p_ref[2 * chans : 3 * chans, :].astype(f32).T.astype(bf16)
    state = jnp.zeros((span, chans), f32)
    for n in range(total // block):
        at_rows = slice(n * block, (n + 1) * block)
        decay = d_s[at_rows, :]
        high = decay.astype(bf16)
        rest = (decay - high.astype(f32)).astype(bf16)
        cum = jnp.dot(tri, high, preferred_element_type=f32) + jnp.dot(
            tri, rest, preferred_element_type=f32
        )
        last = cum[block - 1 : block, :]
        qs = (q_s[at_rows, :] * jnp.exp(cum)).astype(bf16)
        key = k_s[at_rows, :]
        ks = (key * jnp.exp(-cum)).astype(bf16)
        kf = (key * jnp.exp(last - cum)).astype(bf16)
        rows_in = inputs[at_rows, :]
        scores = lax.dot_general(qs, ks, NT, preferred_element_type=f32)
        scores = jnp.where(low, scores, 0.0).astype(bf16)
        r_s[at_rows, :] = jnp.dot(scores, rows_in, preferred_element_type=f32) + jnp.dot(
            qs, state.astype(bf16), preferred_element_type=f32
        )
        state = jnp.exp(last).T * state + lax.dot_general(
            kf, rows_in, TN, preferred_element_type=f32
        )
    rec = r_s[...].T
    outgate = p_ref[3 * chans : 4 * chans, :].astype(f32)
    square = jnp.sum(rec * rec, axis=0, keepdims=True)
    a_ref[chans : 2 * chans, :] = (
        rec * mine[:, width : width + 1] * (outgate * jax.nn.sigmoid(outgate))
    ).astype(bf16)
    upper = square.astype(bf16).astype(f32)
    line = lax.broadcasted_iota(jnp.int32, (a_ref.shape[0] - 2 * chans, total), 0)
    a_ref[2 * chans :, :] = jnp.where(
        line == 0, upper, jnp.where(line == 1, square - upper, 0.0)
    ).astype(bf16)


def output_kernel(
    sizes, a_ref, wo_ref, par_ref, o_ref, held, sums, part, got, mixed, *sems
):
    n_sp, n_tp, rows, chans, members, width, channels = sizes
    send_z, send_x, recv_z, recv_x, send_s, recv_s, send_p, recv_p, send_o, recv_o = sems
    f32, bf16 = jnp.float32, jnp.bfloat16
    s, t = lax.axis_index("sp"), lax.axis_index("tp")
    n_z = n_sp // STRIDE
    z, x = s // STRIDE, s % STRIDE
    x_peer = at(z * STRIDE + (1 - x), t)

    def sp_at(k):
        return lax.rem(s + k, n_sp)

    def tp_at(k):
        return lax.rem(t + k, n_tp)

    greet([at(sp_at(k), t) for k in range(1, n_sp)] + [at(s, tp_at(k)) for k in range(1, n_tp)])
    pending = []

    def launch(copy):
        copy.start()
        pending.append(copy)

    for k in range(1, n_z):
        peer = at(lax.rem(z + k, n_z) * STRIDE + x, t)
        launch(remote(a_ref, held.at[s], send_z.at[k], recv_z.at[k], peer))
    launch(remote(a_ref, held.at[s], send_x.at[0], recv_x.at[0], x_peer))
    held[s] = a_ref[...]
    for k in range(1, n_z):
        source = lax.rem(z - k + n_z, n_z) * STRIDE + x
        here = held.at[source]
        remote(here, here, send_z.at[k], recv_z.at[k], x_peer).wait_recv()
        launch(remote(here, here, send_x.at[k], recv_x.at[k], x_peer))
    for k in range(n_z):
        here = held.at[lax.rem(z - k + n_z, n_z) * STRIDE + (1 - x)]
        remote(here, here, send_x.at[k], recv_x.at[k], x_peer).wait_recv()

    total = a_ref.shape[1]
    conv = held[:, 0:chans, :].reshape(n_sp * chans, total).astype(f32)
    sums[t, 0:1, :] = jnp.sum(conv, axis=0, keepdims=True)
    sums[t, 1:2, :] = jnp.sum(conv * conv, axis=0, keepdims=True)
    for k in range(1, n_tp):
        launch(remote(sums.at[t], sums.at[t], send_s.at[k], recv_s.at[k], at(s, tp_at(k))))
    for k in range(1, n_tp):
        there = sums.at[lax.rem(t - k + n_tp, n_tp)]
        remote(there, there, send_s.at[k], recv_s.at[k], x_peer).wait_recv()
    both = sums[0]
    for k in range(1, n_tp):
        both = both + sums[k]
    mean = both[0:1] / channels
    scale = lax.rsqrt(both[1:2] / channels - mean * mean + layer_eps)
    gain = par_ref[:, width + 2 : width + 3]
    bias = par_ref[:, width + 3 : width + 4]
    span = members * chans
    heads = n_sp // members
    step = rows * n_tp
    for b in range(n_sp):
        lanes = slice(b * step, (b + 1) * step)
        values = held[:, 0:chans, lanes].reshape(n_sp * chans, step).astype(f32)
        shifted = (values - mean[:, lanes]) * scale[:, lanes] * gain + bias
        pieces = [(shifted * jax.nn.sigmoid(shifted)).astype(bf16)]
        for h in range(heads):
            group = slice(h * members, (h + 1) * members)
            square = jnp.sum(held[group, 2 * chans : 2 * chans + 16, lanes].astype(f32), axis=(0, 1), keepdims=True)[0]
            ups = held[group, chans : 2 * chans, lanes].reshape(span, step).astype(f32)
            pieces.append((ups * lax.rsqrt(square / span + norm_eps)).astype(bf16))
        out = lax.dot_general(
            jnp.concatenate(pieces, axis=0), wo_ref[...], TN, preferred_element_type=f32
        ).astype(bf16)
        for k in range(n_tp):
            part[k, b * rows : (b + 1) * rows, :] = out[k * rows : (k + 1) * rows]
    for k in range(1, n_tp):
        launch(remote(part.at[tp_at(k)], got.at[k], send_p.at[k], recv_p.at[k], at(s, tp_at(k))))
    added = part[t].astype(f32)
    for k in range(1, n_tp):
        remote(got.at[k], got.at[k], send_p.at[k], recv_p.at[k], x_peer).wait_recv()
        added = added + got[k].astype(f32)
    mixed[...] = added.astype(bf16)
    cols = wo_ref.shape[1]

    def window(source):
        return o_ref.at[:, pl.ds(pl.multiple_of(source * cols, cols), cols)]

    def block_of(sp):
        return pl.ds(pl.multiple_of(sp * rows, rows), rows)

    for k in range(1, n_sp):
        launch(remote(mixed.at[block_of(sp_at(k))], window(s), send_o.at[k], recv_o.at[k], at(sp_at(k), t)))
    window(s)[...] = mixed[block_of(s), :]
    for k in range(1, n_sp):
        there = window(lax.rem(s - k + n_sp, n_sp))
        remote(there, there, send_o.at[k], recv_o.at[k], x_peer).wait_recv()
    for copy in pending:
        copy.wait_send()


def spread_channels(n_sp, n_tp,
    tokens,
    input_norm_gain,
    convolution_value_weight,
    convolution_gate_weight,
    depthwise_filter_taps,
    channel_norm_gain,
    channel_norm_bias,
    query_projection_weight,
    forget_gate_weight,
    recurrence_value_weight,
    output_gate_weight,
    forget_floor_margin,
    decay_jump_terms,
    head_norm_gain,
    convolution_output_weight,
    recurrence_output_weight,
):
    rows, model = tokens.shape
    total = rows * n_sp * n_tp
    depth, group_chans = convolution_value_weight.shape
    chans = group_chans // n_sp
    heads, part = decay_jump_terms.shape
    members = n_sp // heads
    width = depthwise_filter_taps.shape[0]
    features = tokens.astype(jnp.float32)
    normed = (
        features
        * lax.rsqrt(jnp.mean(features * features, axis=1, keepdims=True) + norm_eps)
        * input_norm_gain
    ).astype(jnp.bfloat16)
    kinds = (
        convolution_value_weight,
        convolution_gate_weight,
        recurrence_value_weight,
        output_gate_weight,
        query_projection_weight,
        forget_gate_weight,
    )
    stacked = jnp.stack([w.T.reshape(n_sp, chans, depth) for w in kinds], axis=1).reshape(
        n_sp, len(kinds) * chans, depth
    )
    jumps = jnp.pad(decay_jump_terms, ((0, -heads % 8), (0, 0)))
    params = jnp.concatenate(
        [
            depthwise_filter_taps.T,
            head_norm_gain[:, None],
            forget_floor_margin[:, None],
            channel_norm_gain[:, None],
            channel_norm_bias[:, None],
        ],
        axis=1,
    )
    weights_out = jnp.concatenate([convolution_output_weight, recurrence_output_weight], axis=0)
    vmem = pl.BlockSpec(memory_space=pltpu.VMEM)
    dma = pltpu.SemaphoreType.DMA
    bf16, f32 = jnp.bfloat16, jnp.float32
    n_z = n_sp // STRIDE
    lanes = 2 * n_sp
    projected, query_forget, all_jumps = pl.pallas_call(
        functools.partial(project_kernel, (n_sp, n_tp, rows, depth, chans, members)),
        out_shape=(
            jax.ShapeDtypeStruct((4 * chans, total), bf16),
            jax.ShapeDtypeStruct((members, 2 * chans, total), bf16),
            jax.ShapeDtypeStruct((n_sp, *jumps.shape), f32),
        ),
        in_specs=[vmem] * 3,
        out_specs=(vmem,) * 3,
        scratch_shapes=[
            pltpu.VMEM((total, model), bf16),
            pltpu.VMEM((len(kinds) * chans, model), bf16),
            dma((n_z,)),
            dma((n_z,)),
            dma((lanes,)),
            dma((lanes,)),
            dma((lanes,)),
            dma((lanes,)),
            dma((n_sp,)),
            dma((n_sp,)),
            dma((n_sp,)),
            dma((n_sp,)),
            dma((members,)),
            dma((members,)),
        ],
        compiler_params=pltpu.CompilerParams(collective_id=0, has_side_effects=True),
        name="project",
    )(normed, stacked, jumps)
    span = members * chans
    sent = pl.pallas_call(
        functools.partial(mix_kernel, (n_sp, chans, members, width, HG_BLOCK, part)),
        out_shape=jax.ShapeDtypeStruct((2 * chans + 16, total), bf16),
        in_specs=[vmem] * 4,
        out_specs=vmem,
        scratch_shapes=[pltpu.VMEM((total, span), f32)] * 3 + [pltpu.VMEM((total, chans), f32)],
        name="mix",
    )(projected, query_forget, all_jumps, params)
    cols = weights_out.shape[1]
    return pl.pallas_call(
        functools.partial(
            output_kernel, (n_sp, n_tp, rows, chans, members, width, group_chans * n_tp)
        ),
        out_shape=jax.ShapeDtypeStruct((rows, model), bf16),
        in_specs=[vmem] * 3,
        out_specs=vmem,
        scratch_shapes=[
            pltpu.VMEM((n_sp, 2 * chans + 16, total), bf16),
            pltpu.VMEM((n_tp, 8, total), f32),
            pltpu.VMEM((n_tp, n_sp * rows, cols), bf16),
            pltpu.VMEM((n_tp, n_sp * rows, cols), bf16),
            pltpu.VMEM((n_sp * rows, cols), bf16),
            dma((n_z,)),
            dma((n_z,)),
            dma((n_z,)),
            dma((n_z,)),
            dma((n_tp,)),
            dma((n_tp,)),
            dma((n_tp,)),
            dma((n_tp,)),
            dma((n_sp,)),
            dma((n_sp,)),
        ],
        compiler_params=pltpu.CompilerParams(collective_id=1, has_side_effects=True),
        name="output",
    )(sent, weights_out, params)


def layer(n_sp, n_tp, *arrays):
    rows, model = arrays[0].shape
    group_chans = arrays[2].shape[1]
    heads = arrays[12].shape[0]
    gathered_bytes = rows * n_sp * n_tp * model * arrays[0].dtype.itemsize
    fits = gathered_bytes <= 2**23
    even = n_tp == 4 and n_sp % heads == 0 and n_sp % STRIDE == 0 and group_chans % (32 * n_sp) == 0
    if fits and even:
        return spread_channels(n_sp, n_tp, *arrays)
    return per_device(*arrays)


def solution(mesh):
    in_specs = (
        P(("sp", "tp"), None),
        P(),
        P("sp", "tp"),
        P("sp", "tp"),
        P(None, "tp"),
        P("tp"),
        P("tp"),
        P("sp", "tp"),
        P("sp", "tp"),
        P("sp", "tp"),
        P("sp", "tp"),
        P("tp"),
        P("tp", "sp"),
        P("tp"),
        P("tp", "sp"),
        P("tp", "sp"),
    )
    out_specs = P(("sp", "tp"), None)
    return jax.shard_map(
        functools.partial(layer, mesh.shape["sp"], mesh.shape["tp"]), mesh=mesh, in_specs=in_specs, out_specs=out_specs, check_vma=False
    )
```

```python
import functools

import jax
import jax.numpy as jnp
from jax import lax
from jax.experimental import pallas as pl
from jax.experimental.pallas import tpu as pltpu
from jax.sharding import PartitionSpec as P

CONV_CH = 1024
HG_DK = 128
HG_DV = 128
HG_BLOCK = 64


norm_eps = 1e-06
layer_eps = 1e-05
highest_precision = lax.Precision.HIGHEST


def passed_along(value, axis, steps):
    count = lax.axis_size(axis)
    initial, last = (max(0, -steps), min(count, count - steps))
    return lax.ppermute(value, axis, [(source, source + steps) for source in range(initial, last)])


def prefix(x, axis, combine, identity):
    size, mine = (lax.axis_size(axis), lax.axis_index(axis))
    everything = jax.tree.map(
        lambda part, kind: lax.all_gather(part.astype(kind), axis), x, (jnp.bfloat16, jnp.bfloat16)
    )
    start = jax.tree.map(
        lambda part, zero: jnp.broadcast_to(jnp.asarray(zero, part.dtype), part.shape), x, identity
    )

    def lap(k, before):
        reached = k < mine
        new = combine(
            before, jax.tree.map(lambda part, own: part[k].astype(own.dtype), everything, x)
        )
        return jax.tree.map(lambda a, b: jnp.where(reached, a, b), new, before)

    return lax.fori_loop(0, size, lap, start)


def convolve(gated, kernel):
    return lax.conv_general_dilated(
        gated[None],
        kernel[:, None, :],
        (1,),
        "VALID",
        dimension_numbers=("NWC", "WIO", "NWC"),
        feature_group_count=gated.shape[1],
        precision=highest_precision,
    )[0]


def channel_norm(values, first_sum, second_sum, gain, bias):
    mean_value = first_sum[:, None] / CONV_CH
    variance = second_sum[:, None] / CONV_CH - mean_value * mean_value
    shifted = (values - mean_value) * lax.rsqrt(variance + layer_eps) * gain + bias
    return jax.nn.silu(shifted).astype(jnp.bfloat16)


def gate_factors(query_projected, forget_projected, forget_floor_margin, decay_jump_rows):
    row_total_count = query_projected.shape[0]
    head_total_count = decay_jump_rows.shape[1]
    query_rows = jax.nn.silu(query_projected.astype(jnp.float32))
    log_forget_gate = jnp.logaddexp(
        jnp.log1p(-forget_floor_margin),
        jnp.log(forget_floor_margin) + jax.nn.log_sigmoid(forget_projected.astype(jnp.float32)),
    )
    key_gate_values = -jnp.expm1(log_forget_gate)
    log_decay_running = (
        log_forget_gate.reshape(row_total_count, head_total_count, -1) + decay_jump_rows[:, :, None]
    )
    return (
        query_rows.reshape(row_total_count, head_total_count, -1),
        key_gate_values.reshape(row_total_count, head_total_count, -1),
        log_decay_running,
    )


def finish(recurrent, gain, outgate_proj):
    row_total_count = recurrent.shape[0]
    scaled = recurrent * lax.rsqrt(
        jnp.mean(recurrent * recurrent, axis=2, keepdims=True) + norm_eps
    )
    gated_out = (
        scaled.reshape(row_total_count, -1) * gain * jax.nn.silu(outgate_proj.astype(jnp.float32))
    )
    return gated_out.astype(jnp.bfloat16)


def combine_states(first_part, second_part):
    return (
        first_part[0] + second_part[0],
        jnp.exp(second_part[0])[:, :, None] * first_part[1] + second_part[1],
    )


def carry_step(recurrence_state, block_parts):
    decay_end, contribution = block_parts
    return (jnp.exp(decay_end)[:, :, None] * recurrence_state + contribution, recurrence_state)


def per_device(
    tokens,
    input_norm_gain,
    convolution_value_weight,
    convolution_gate_weight,
    depthwise_filter_taps,
    channel_norm_gain,
    channel_norm_bias,
    query_projection_weight,
    forget_gate_weight,
    recurrence_value_weight,
    output_gate_weight,
    forget_floor_margin,
    decay_jump_terms,
    head_norm_gain,
    convolution_output_weight,
    recurrence_output_weight,
):
    features = tokens.astype(jnp.float32)
    normed = (
        features
        * lax.rsqrt(jnp.mean(features * features, axis=1, keepdims=True) + norm_eps)
        * input_norm_gain
    ).astype(jnp.bfloat16)
    gathered = (
        lax.all_gather(convolution_value_weight, "sp", axis=0, tiled=True),
        lax.all_gather(convolution_gate_weight, "sp", axis=0, tiled=True),
        lax.all_gather(query_projection_weight, "sp", axis=0, tiled=True),
        lax.all_gather(forget_gate_weight, "sp", axis=0, tiled=True),
        lax.all_gather(recurrence_value_weight, "sp", axis=0, tiled=True),
        lax.all_gather(output_gate_weight, "sp", axis=0, tiled=True),
        lax.all_gather(convolution_output_weight, "sp", axis=1, tiled=True),
        lax.all_gather(recurrence_output_weight, "sp", axis=1, tiled=True),
    )
    projection_weights = gathered[:6]
    conv_columns = gathered[6]
    rec_columns = gathered[7]

    def project(row_piece):
        return jnp.concatenate(
            [
                jnp.dot(row_piece, weight, preferred_element_type=jnp.float32).astype(jnp.bfloat16)
                for weight in projection_weights
            ],
            axis=1,
        )

    projected = project(lax.all_gather(normed, "tp", axis=0, tiled=True))
    offsets = []
    position = 0
    for weight in projection_weights[:-1]:
        position = position + weight.shape[1]
        offsets.append(position)
    value_proj, gate_proj, query_projected, forget_projected, input_proj, outgate_proj = jnp.split(
        projected, offsets, axis=1
    )
    row_total_count = value_proj.shape[0]
    rim_rows = depthwise_filter_taps.shape[0] - 1
    tail_value, tail_gate = passed_along(
        (value_proj[row_total_count - rim_rows :], gate_proj[row_total_count - rim_rows :]), "sp", 1
    )
    value_ext = jnp.concatenate([tail_value, value_proj], axis=0)
    gate_ext = jnp.concatenate([tail_gate, gate_proj], axis=0)
    gated = value_ext.astype(jnp.float32) * jax.nn.sigmoid(gate_ext.astype(jnp.float32))
    convolved = convolve(gated, depthwise_filter_taps).astype(jnp.bfloat16)
    device_heads = decay_jump_terms.shape[0]
    query_rows, key_gate_values, log_decay_running = gate_factors(
        query_projected, forget_projected, forget_floor_margin, decay_jump_terms.T
    )
    input_rows = input_proj.astype(jnp.float32).reshape(row_total_count, device_heads, -1)
    block_count = row_total_count // HG_BLOCK

    def to_blocks(array):
        return array.reshape(block_count, HG_BLOCK, device_heads, -1).transpose(0, 2, 1, 3)

    block_queries = to_blocks(query_rows)
    block_keys = to_blocks(key_gate_values)
    block_inputs = to_blocks(input_rows)
    cumulative = jnp.cumsum(to_blocks(log_decay_running), axis=2)
    final_decay = cumulative[:, :, -1, :]
    query_rows_scaled = block_queries * jnp.exp(cumulative)
    scaled_keys = block_keys * jnp.exp(-cumulative)
    final_keys = block_keys * jnp.exp(final_decay[:, :, None, :] - cumulative)
    attention_scores = jnp.einsum(
        "nhtk,nhsk->nhts", query_rows_scaled, scaled_keys, precision=highest_precision
    )
    causal = jnp.arange(HG_BLOCK)[:, None] >= jnp.arange(HG_BLOCK)[None, :]
    attention_scores = jnp.where(causal[None, None], attention_scores, 0.0)
    inner = jnp.einsum(
        "nhts,nhsv->nhtv", attention_scores, block_inputs, precision=highest_precision
    )
    contributions = jnp.einsum(
        "nhsk,nhsv->nhkv", final_keys, block_inputs, precision=highest_precision
    )
    initial = jnp.zeros((device_heads, HG_DK, HG_DV), jnp.float32)
    local_state, block_starts = lax.scan(carry_step, initial, (final_decay, contributions))
    device_decay = jnp.sum(final_decay, axis=0)
    before_blocks = jnp.cumsum(final_decay, axis=0) - final_decay
    incoming = prefix(
        (device_decay, local_state),
        "sp",
        combine_states,
        (jnp.zeros_like(device_decay), jnp.zeros_like(local_state)),
    )
    starts = block_starts + jnp.exp(before_blocks)[:, :, :, None] * incoming[1][None]
    recurrent = inner + jnp.einsum(
        "nhtk,nhkv->nhtv", query_rows_scaled, starts, precision=highest_precision
    )
    recurrent = recurrent.transpose(0, 2, 1, 3).reshape(row_total_count, device_heads, -1)
    rec_out = finish(recurrent, head_norm_gain, outgate_proj)
    values = convolved.astype(jnp.float32)
    totals = lax.psum((jnp.sum(values, axis=1), jnp.sum(values * values, axis=1)), "tp")
    conv_out = channel_norm(values, totals[0], totals[1], channel_norm_gain, channel_norm_bias)
    conv_part = lax.slice_in_dim(
        conv_out, 0, row_total_count // lax.axis_size("tp") * lax.axis_size("tp"), axis=0
    )
    return lax.psum_scatter(
        (
            jnp.dot(conv_part, conv_columns, preferred_element_type=jnp.float32)
            + jnp.dot(rec_out, rec_columns, preferred_element_type=jnp.float32)
        ).astype(jnp.bfloat16),
        "tp",
        scatter_dimension=0,
        tiled=True,
    )


MESH = pl.DeviceIdType.MESH
STRIDE = 2
NT = (((1,), (1,)), ((), ()))
TN = (((0,), (0,)), ((), ()))


def at(sp, tp):
    return {"sp": sp, "tp": tp}


def greet(peers):
    barrier = pltpu.get_barrier_semaphore()
    for peer in peers:
        pl.semaphore_signal(barrier, inc=1, device_id=peer, device_id_type=MESH)
    pl.semaphore_wait(barrier, len(peers))


def remote(src, dst, send, recv, peer):
    return pltpu.make_async_remote_copy(
        src_ref=src, dst_ref=dst, send_sem=send, recv_sem=recv, device_id=peer, device_id_type=MESH
    )


def project_kernel(
    sizes, x_hbm, gain_ref, j_ref, cv, cg, rv, og, qw, fw, p_ref, qf_ref, jump_ref,
    x_ref, raw, w_ref, held, weights, load, *sems
):
    n_sp, n_tp, rows, depth, chans, members = sizes
    (send_z, send_x, send_y, send_c, lane, sib, send_w, recv_w, send_j, recv_j, send_q, recv_q) = sems
    s, t = lax.axis_index("sp"), lax.axis_index("tp")
    n_z = n_sp // STRIDE
    z, x = s // STRIDE, s % STRIDE
    y, c = t // 2, t % 2
    x_peer = at(z * STRIDE + (1 - x), t)
    y_peer = at(s, (1 - y) * 2 + c)
    c_peer = at(s, y * 2 + (1 - c))
    total = held.shape[0]
    half = total // 2

    def sp_peer(k):
        return lax.rem(s + k, n_sp)

    def slot(dy, dx, dz, core):
        from_z = lax.rem(z - dz + n_z, n_z)
        from_x = (1 - x) if dx else x
        from_y = (1 - y) if dy else y
        start = from_y * half + ((from_z * STRIDE + from_x) * 2 + core) * rows
        return pl.ds(pl.multiple_of(start, rows), rows)

    def number(dy, dx, dz):
        return (dy * STRIDE + dx) * n_z + dz

    peers = [at(sp_peer(k), t) for k in range(1, n_sp)] + [y_peer, c_peer]
    barrier = pltpu.get_barrier_semaphore()
    for peer in peers:
        pl.semaphore_signal(barrier, inc=1, device_id=peer, device_id_type=MESH)
    kinds = (cv, cg, rv, og, qw, fw)
    loads = [pltpu.make_async_copy(x_hbm, x_ref, load.at[0])] + [
        pltpu.make_async_copy(w, raw.at[i], load.at[1 + i]) for i, w in enumerate(kinds)
    ]
    for copy in loads:
        copy.start()
    own = slot(0, 0, 0, c)
    mine = held.at[own]
    loads[0].wait()
    features = x_ref[...].astype(jnp.float32)
    mine[...] = (
        features
        * lax.rsqrt(jnp.mean(features * features, axis=1, keepdims=True) + norm_eps)
        * gain_ref[...]
    ).astype(jnp.bfloat16)
    pl.semaphore_wait(barrier, len(peers))
    pending = []

    def launch(copy):
        copy.start()
        pending.append(copy)

    def pass_on(dy, dx, dz):
        here = held.at[slot(dy, dx, dz, c)]
        at_number = number(dy, dx, dz)
        if not dy:
            if not dx:
                launch(remote(here, here, send_x.at[dz], lane.at[number(0, 1, dz)], x_peer))
            launch(remote(here, here, send_y.at[at_number], lane.at[number(1, dx, dz)], y_peer))
        launch(remote(here, here, send_c.at[at_number], sib.at[at_number], c_peer))

    near_first = sorted(range(1, n_z), key=lambda k: min(k, n_z - k))
    for k in near_first:
        peer = at(lax.rem(z + k, n_z) * STRIDE + x, t)
        launch(remote(mine, mine, send_z.at[k], lane.at[k], peer))
    pass_on(0, 0, 0)
    for k in range(1, n_sp):
        launch(remote(j_ref, jump_ref.at[s], send_j.at[k], recv_j.at[k], at(sp_peer(k), t)))
    jump_ref[s] = j_ref[...]
    for i in range(len(kinds)):
        loads[1 + i].wait()
        turned = raw[i].T
        for d in range(n_sp):
            w_ref[d, i * chans : (i + 1) * chans, :] = turned[d * chans : (d + 1) * chans]
    my_columns = pl.ds(pl.multiple_of(s * depth, depth), depth)

    def send_weights(dx, dz):
        other = lax.rem(z + dz, n_z) * STRIDE + ((1 - x) if dx else x)
        k = dx * n_z + dz
        launch(remote(w_ref.at[other], weights.at[:, my_columns], send_w.at[k], recv_w.at[k], at(other, t)))

    for dz in near_first:
        send_weights(0, dz)
    weights[:, my_columns] = w_ref[s]

    def arrived(dy, dx, dz):
        here = held.at[slot(dy, dx, dz, c)]
        remote(here, here, send_c.at[0], lane.at[number(dy, dx, dz)], c_peer).wait_recv()
        pass_on(dy, dx, dz)

    order = []
    for dz in near_first:
        order += [(0, dz), (1, 0 if dz == near_first[0] else order[-2][1])]
    order.append((1, near_first[-1]))
    for dx, dz in order:
        arrived(0, dx, dz)
    for dz in [0] + near_first:
        send_weights(1, dz)
    across = [(0, 0)] + order
    early = len(across) // 2 + 1
    for dx, dz in across[:early]:
        arrived(1, dx, dz)
    for dx in range(STRIDE):
        for dz in range(n_z):
            if dx or dz:
                source = lax.rem(z - dz + n_z, n_z) * STRIDE + ((1 - x) if dx else x)
                there = weights.at[:, pl.ds(pl.multiple_of(source * depth, depth), depth)]
                k = dx * n_z + dz
                remote(there, there, send_w.at[k], recv_w.at[k], c_peer).wait_recv()
    member = lax.rem(s, members)
    first = s - member

    def project_half(dy):
        for dx in range(STRIDE):
            for dz in range(n_z):
                here = held.at[slot(dy, dx, dz, 1 - c)]
                remote(here, here, send_c.at[0], sib.at[number(dy, dx, dz)], c_peer).wait_recv()
        base = ((1 - y) if dy else y) * half
        step = min(256, half)
        for start in range(0, half, step):
            span = pl.ds(pl.multiple_of(base + start, step), step)
            piece = lax.dot_general(
                held[span, :], weights[...], NT, preferred_element_type=jnp.float32
            ).T.astype(jnp.bfloat16)
            qf_ref[member, :, span] = piece[4 * chans :]
            p_ref[:, span] = piece[: 4 * chans]
        window = pl.ds(pl.multiple_of(base, half), half)
        for k in range(1, members):
            peer = at(first + lax.rem(member + k, members), t)
            block = qf_ref.at[member, :, window]
            launch(remote(block, block, send_q.at[dy, k], recv_q.at[dy, k], peer))

    project_half(0)
    for dx, dz in across[early:]:
        arrived(1, dx, dz)
    project_half(1)
    for dy in range(2):
        window = pl.ds(pl.multiple_of(((1 - y) if dy else y) * half, half), half)
        for k in range(1, members):
            there = qf_ref.at[lax.rem(member - k + members, members), :, window]
            remote(there, there, send_q.at[dy, k], recv_q.at[dy, k], c_peer).wait_recv()
    for k in range(1, n_sp):
        there = jump_ref.at[lax.rem(s - k + n_sp, n_sp)]
        remote(there, there, send_j.at[k], recv_j.at[k], c_peer).wait_recv()
    for copy in pending:
        copy.wait_send()


def in_order(array, n_sp):
    half = array.shape[1] // 2
    own = half // n_sp
    return jnp.concatenate(
        [
            array[:, side * half + b * own : side * half + (b + 1) * own]
            for b in range(n_sp)
            for side in range(2)
        ],
        axis=1,
    )


def mix_kernel(sizes, p_ref, qf_ref, jump_ref, par_ref, a_ref, q_s, k_s, d_s, r_s):
    n_sp, chans, members, width, block, part = sizes
    s = lax.axis_index("sp")
    total = p_ref.shape[1]
    f32, bf16 = jnp.float32, jnp.bfloat16
    mine = par_ref[pl.ds(pl.multiple_of(s * chans, chans), chans), :]
    head = s // members
    span = chans * members
    margin = par_ref[pl.ds(pl.multiple_of(head * span, span), span), width + 1 : width + 2]

    projected = in_order(p_ref[...].astype(f32), n_sp)
    value = projected[0:chans]
    gate = projected[chans : 2 * chans]
    gated = value * jax.nn.sigmoid(gate)
    place = lax.broadcasted_iota(jnp.int32, gated.shape, 1)
    conv = gated * mine[:, width - 1 : width]
    for back in range(1, width):
        moved = jnp.where(place >= back, pltpu.roll(gated, back, 1), 0.0)
        conv = conv + moved * mine[:, width - 1 - back : width - back]
    a_ref[0:chans, :] = conv.astype(bf16)

    picked = lax.broadcasted_iota(jnp.int32, jump_ref.shape[1:], 0) == head
    arranged = [in_order(qf_ref[m].astype(f32), n_sp) for m in range(members)]
    for b in range(n_sp):
        lanes = slice(b * part, (b + 1) * part)
        jump = jnp.sum(jnp.where(picked, jump_ref[b], 0.0), axis=0, keepdims=True)
        both = [arranged[m][:, lanes] for m in range(members)]
        query = jnp.concatenate([v[:chans] for v in both], axis=0)
        forget = jnp.concatenate([v[chans:] for v in both], axis=0)
        key = margin * jax.nn.sigmoid(-forget)
        q_s[lanes, :] = (query * jax.nn.sigmoid(query)).T
        k_s[lanes, :] = key.T
        d_s[lanes, :] = (jnp.log1p(-key) + jump).T
    low = lax.broadcasted_iota(jnp.int32, (block, block), 0) >= lax.broadcasted_iota(
        jnp.int32, (block, block), 1
    )
    tri = low.astype(bf16)
    inputs = projected[2 * chans : 3 * chans].T.astype(bf16)
    state = jnp.zeros((span, chans), f32)
    for n in range(total // block):
        at_rows = slice(n * block, (n + 1) * block)
        decay = d_s[at_rows, :]
        high = decay.astype(bf16)
        rest = (decay - high.astype(f32)).astype(bf16)
        cum = jnp.dot(tri, high, preferred_element_type=f32) + jnp.dot(
            tri, rest, preferred_element_type=f32
        )
        last = cum[block - 1 : block, :]
        qs = (q_s[at_rows, :] * jnp.exp(cum)).astype(bf16)
        key = k_s[at_rows, :]
        ks = (key * jnp.exp(-cum)).astype(bf16)
        kf = (key * jnp.exp(last - cum)).astype(bf16)
        rows_in = inputs[at_rows, :]
        scores = lax.dot_general(qs, ks, NT, preferred_element_type=f32)
        scores = jnp.where(low, scores, 0.0).astype(bf16)
        r_s[at_rows, :] = jnp.dot(scores, rows_in, preferred_element_type=f32) + jnp.dot(
            qs, state.astype(bf16), preferred_element_type=f32
        )
        state = jnp.exp(last).T * state + lax.dot_general(
            kf, rows_in, TN, preferred_element_type=f32
        )
    rec = r_s[...].T
    outgate = projected[3 * chans : 4 * chans]
    square = jnp.sum(rec * rec, axis=0, keepdims=True)
    a_ref[chans : 2 * chans, :] = (
        rec * mine[:, width : width + 1] * (outgate * jax.nn.sigmoid(outgate))
    ).astype(bf16)
    upper = square.astype(bf16).astype(f32)
    line = lax.broadcasted_iota(jnp.int32, (a_ref.shape[0] - 2 * chans, total), 0)
    a_ref[2 * chans :, :] = jnp.where(
        line == 0, upper, jnp.where(line == 1, square - upper, 0.0)
    ).astype(bf16)


def output_kernel(
    sizes, a_ref, wo_ref, par_ref, o_ref, held, sums, part, got, mixed, *sems
):
    n_sp, n_tp, rows, chans, members, width, channels = sizes
    send_z, send_x, recv_z, recv_x, send_s, recv_s, send_p, recv_p, send_o, recv_o = sems
    f32, bf16 = jnp.float32, jnp.bfloat16
    s, t = lax.axis_index("sp"), lax.axis_index("tp")
    n_z = n_sp // STRIDE
    z, x = s // STRIDE, s % STRIDE
    x_peer = at(z * STRIDE + (1 - x), t)

    def sp_at(k):
        return lax.rem(s + k, n_sp)

    def tp_at(k):
        return lax.rem(t + k, n_tp)

    greet([at(sp_at(k), t) for k in range(1, n_sp)] + [at(s, tp_at(k)) for k in range(1, n_tp)])
    pending = []

    def launch(copy):
        copy.start()
        pending.append(copy)

    for k in range(1, n_z):
        peer = at(lax.rem(z + k, n_z) * STRIDE + x, t)
        launch(remote(a_ref, held.at[s], send_z.at[k], recv_z.at[k], peer))
    launch(remote(a_ref, held.at[s], send_x.at[0], recv_x.at[0], x_peer))
    held[s] = a_ref[...]
    for k in range(1, n_z):
        source = lax.rem(z - k + n_z, n_z) * STRIDE + x
        here = held.at[source]
        remote(here, here, send_z.at[k], recv_z.at[k], x_peer).wait_recv()
        launch(remote(here, here, send_x.at[k], recv_x.at[k], x_peer))
    for k in range(n_z):
        here = held.at[lax.rem(z - k + n_z, n_z) * STRIDE + (1 - x)]
        remote(here, here, send_x.at[k], recv_x.at[k], x_peer).wait_recv()

    total = a_ref.shape[1]
    conv = held[:, 0:chans, :].reshape(n_sp * chans, total).astype(f32)
    sums[t, 0:1, :] = jnp.sum(conv, axis=0, keepdims=True)
    sums[t, 1:2, :] = jnp.sum(conv * conv, axis=0, keepdims=True)
    for k in range(1, n_tp):
        launch(remote(sums.at[t], sums.at[t], send_s.at[k], recv_s.at[k], at(s, tp_at(k))))
    for k in range(1, n_tp):
        there = sums.at[lax.rem(t - k + n_tp, n_tp)]
        remote(there, there, send_s.at[k], recv_s.at[k], x_peer).wait_recv()
    both = sums[0]
    for k in range(1, n_tp):
        both = both + sums[k]
    mean = both[0:1] / channels
    scale = lax.rsqrt(both[1:2] / channels - mean * mean + layer_eps)
    gain = par_ref[:, width + 2 : width + 3]
    bias = par_ref[:, width + 3 : width + 4]
    span = members * chans
    heads = n_sp // members
    step = rows * n_tp
    for b in range(n_sp):
        lanes = slice(b * step, (b + 1) * step)
        values = held[:, 0:chans, lanes].reshape(n_sp * chans, step).astype(f32)
        shifted = (values - mean[:, lanes]) * scale[:, lanes] * gain + bias
        pieces = [(shifted * jax.nn.sigmoid(shifted)).astype(bf16)]
        for h in range(heads):
            group = slice(h * members, (h + 1) * members)
            square = jnp.sum(held[group, 2 * chans : 2 * chans + 16, lanes].astype(f32), axis=(0, 1), keepdims=True)[0]
            ups = held[group, chans : 2 * chans, lanes].reshape(span, step).astype(f32)
            pieces.append((ups * lax.rsqrt(square / span + norm_eps)).astype(bf16))
        out = lax.dot_general(
            jnp.concatenate(pieces, axis=0), wo_ref[...], TN, preferred_element_type=f32
        ).astype(bf16)
        for k in range(n_tp):
            part[k, b * rows : (b + 1) * rows, :] = out[k * rows : (k + 1) * rows]
    for k in range(1, n_tp):
        launch(remote(part.at[tp_at(k)], got.at[k], send_p.at[k], recv_p.at[k], at(s, tp_at(k))))
    added = part[t].astype(f32)
    for k in range(1, n_tp):
        remote(got.at[k], got.at[k], send_p.at[k], recv_p.at[k], x_peer).wait_recv()
        added = added + got[k].astype(f32)
    mixed[...] = added.astype(bf16)
    cols = wo_ref.shape[1]

    def window(source):
        return o_ref.at[:, pl.ds(pl.multiple_of(source * cols, cols), cols)]

    def block_of(sp):
        return pl.ds(pl.multiple_of(sp * rows, rows), rows)

    for k in range(1, n_sp):
        launch(remote(mixed.at[block_of(sp_at(k))], window(s), send_o.at[k], recv_o.at[k], at(sp_at(k), t)))
    window(s)[...] = mixed[block_of(s), :]
    for k in range(1, n_sp):
        there = window(lax.rem(s - k + n_sp, n_sp))
        remote(there, there, send_o.at[k], recv_o.at[k], x_peer).wait_recv()
    for copy in pending:
        copy.wait_send()


def spread_channels(n_sp, n_tp,
    tokens,
    input_norm_gain,
    convolution_value_weight,
    convolution_gate_weight,
    depthwise_filter_taps,
    channel_norm_gain,
    channel_norm_bias,
    query_projection_weight,
    forget_gate_weight,
    recurrence_value_weight,
    output_gate_weight,
    forget_floor_margin,
    decay_jump_terms,
    head_norm_gain,
    convolution_output_weight,
    recurrence_output_weight,
):
    rows, model = tokens.shape
    total = rows * n_sp * n_tp
    depth, group_chans = convolution_value_weight.shape
    chans = group_chans // n_sp
    heads, part = decay_jump_terms.shape
    members = n_sp // heads
    width = depthwise_filter_taps.shape[0]
    kinds = (
        convolution_value_weight,
        convolution_gate_weight,
        recurrence_value_weight,
        output_gate_weight,
        query_projection_weight,
        forget_gate_weight,
    )
    jumps = jnp.pad(decay_jump_terms, ((0, -heads % 8), (0, 0)))
    params = jnp.concatenate(
        [
            depthwise_filter_taps.T,
            head_norm_gain[:, None],
            forget_floor_margin[:, None],
            channel_norm_gain[:, None],
            channel_norm_bias[:, None],
        ],
        axis=1,
    )
    weights_out = jnp.concatenate([convolution_output_weight, recurrence_output_weight], axis=0)
    vmem = pl.BlockSpec(memory_space=pltpu.VMEM)
    anywhere = pl.BlockSpec(memory_space=pl.ANY)
    dma = pltpu.SemaphoreType.DMA
    bf16, f32 = jnp.bfloat16, jnp.float32
    n_z = n_sp // STRIDE
    lanes = 2 * n_sp
    projected, query_forget, all_jumps = pl.pallas_call(
        functools.partial(project_kernel, (n_sp, n_tp, rows, depth, chans, members)),
        out_shape=(
            jax.ShapeDtypeStruct((4 * chans, total), bf16),
            jax.ShapeDtypeStruct((members, 2 * chans, total), bf16),
            jax.ShapeDtypeStruct((n_sp, *jumps.shape), f32),
        ),
        in_specs=[anywhere, vmem, vmem] + [anywhere] * len(kinds),
        out_specs=(vmem,) * 3,
        scratch_shapes=[
            pltpu.VMEM((rows, model), bf16),
            pltpu.VMEM((len(kinds), depth, group_chans), bf16),
            pltpu.VMEM((n_sp, len(kinds) * chans, depth), bf16),
            pltpu.VMEM((total, model), bf16),
            pltpu.VMEM((len(kinds) * chans, model), bf16),
            dma((1 + len(kinds),)),
            dma((n_z,)),
            dma((n_z,)),
            dma((lanes,)),
            dma((lanes,)),
            dma((lanes,)),
            dma((lanes,)),
            dma((n_sp,)),
            dma((n_sp,)),
            dma((n_sp,)),
            dma((n_sp,)),
            dma((2, members)),
            dma((2, members)),
        ],
        compiler_params=pltpu.CompilerParams(collective_id=0, has_side_effects=True),
        name="project",
    )(tokens, input_norm_gain[None, :], jumps, *kinds)
    span = members * chans
    sent = pl.pallas_call(
        functools.partial(mix_kernel, (n_sp, chans, members, width, HG_BLOCK, part)),
        out_shape=jax.ShapeDtypeStruct((2 * chans + 16, total), bf16),
        in_specs=[vmem] * 4,
        out_specs=vmem,
        scratch_shapes=[pltpu.VMEM((total, span), f32)] * 3 + [pltpu.VMEM((total, chans), f32)],
        name="mix",
    )(projected, query_forget, all_jumps, params)
    cols = weights_out.shape[1]
    return pl.pallas_call(
        functools.partial(
            output_kernel, (n_sp, n_tp, rows, chans, members, width, group_chans * n_tp)
        ),
        out_shape=jax.ShapeDtypeStruct((rows, model), bf16),
        in_specs=[vmem] * 3,
        out_specs=vmem,
        scratch_shapes=[
            pltpu.VMEM((n_sp, 2 * chans + 16, total), bf16),
            pltpu.VMEM((n_tp, 8, total), f32),
            pltpu.VMEM((n_tp, n_sp * rows, cols), bf16),
            pltpu.VMEM((n_tp, n_sp * rows, cols), bf16),
            pltpu.VMEM((n_sp * rows, cols), bf16),
            dma((n_z,)),
            dma((n_z,)),
            dma((n_z,)),
            dma((n_z,)),
            dma((n_tp,)),
            dma((n_tp,)),
            dma((n_tp,)),
            dma((n_tp,)),
            dma((n_sp,)),
            dma((n_sp,)),
        ],
        compiler_params=pltpu.CompilerParams(collective_id=1, has_side_effects=True),
        name="output",
    )(sent, weights_out, params)


def layer(n_sp, n_tp, *arrays):
    rows, model = arrays[0].shape
    group_chans = arrays[2].shape[1]
    heads = arrays[12].shape[0]
    gathered_bytes = rows * n_sp * n_tp * model * arrays[0].dtype.itemsize
    fits = gathered_bytes <= 2**23
    even = n_tp == 4 and n_sp % heads == 0 and n_sp % STRIDE == 0 and group_chans % (32 * n_sp) == 0
    if fits and even:
        return spread_channels(n_sp, n_tp, *arrays)
    return per_device(*arrays)


def solution(mesh):
    in_specs = (
        P(("sp", "tp"), None),
        P(),
        P("sp", "tp"),
        P("sp", "tp"),
        P(None, "tp"),
        P("tp"),
        P("tp"),
        P("sp", "tp"),
        P("sp", "tp"),
        P("sp", "tp"),
        P("sp", "tp"),
        P("tp"),
        P("tp", "sp"),
        P("tp"),
        P("tp", "sp"),
        P("tp", "sp"),
    )
    out_specs = P(("sp", "tp"), None)
    return jax.shard_map(
        functools.partial(layer, mesh.shape["sp"], mesh.shape["tp"]), mesh=mesh, in_specs=in_specs, out_specs=out_specs, check_vma=False
    )
```

```python
import functools

import jax
import jax.numpy as jnp
from jax import lax
from jax.experimental import pallas as pl
from jax.experimental.pallas import tpu as pltpu
from jax.sharding import PartitionSpec as P

CONV_CH = 1024
HG_DK = 128
HG_DV = 128
HG_BLOCK = 64


norm_eps = 1e-06
layer_eps = 1e-05
highest_precision = lax.Precision.HIGHEST


def passed_along(value, axis, steps):
    count = lax.axis_size(axis)
    initial, last = (max(0, -steps), min(count, count - steps))
    return lax.ppermute(value, axis, [(source, source + steps) for source in range(initial, last)])


def prefix(x, axis, combine, identity):
    size, mine = (lax.axis_size(axis), lax.axis_index(axis))
    everything = jax.tree.map(
        lambda part, kind: lax.all_gather(part.astype(kind), axis), x, (jnp.bfloat16, jnp.bfloat16)
    )
    start = jax.tree.map(
        lambda part, zero: jnp.broadcast_to(jnp.asarray(zero, part.dtype), part.shape), x, identity
    )

    def lap(k, before):
        reached = k < mine
        new = combine(
            before, jax.tree.map(lambda part, own: part[k].astype(own.dtype), everything, x)
        )
        return jax.tree.map(lambda a, b: jnp.where(reached, a, b), new, before)

    return lax.fori_loop(0, size, lap, start)


def convolve(gated, kernel):
    return lax.conv_general_dilated(
        gated[None],
        kernel[:, None, :],
        (1,),
        "VALID",
        dimension_numbers=("NWC", "WIO", "NWC"),
        feature_group_count=gated.shape[1],
        precision=highest_precision,
    )[0]


def channel_norm(values, first_sum, second_sum, gain, bias):
    mean_value = first_sum[:, None] / CONV_CH
    variance = second_sum[:, None] / CONV_CH - mean_value * mean_value
    shifted = (values - mean_value) * lax.rsqrt(variance + layer_eps) * gain + bias
    return jax.nn.silu(shifted).astype(jnp.bfloat16)


def gate_factors(query_projected, forget_projected, forget_floor_margin, decay_jump_rows):
    row_total_count = query_projected.shape[0]
    head_total_count = decay_jump_rows.shape[1]
    query_rows = jax.nn.silu(query_projected.astype(jnp.float32))
    log_forget_gate = jnp.logaddexp(
        jnp.log1p(-forget_floor_margin),
        jnp.log(forget_floor_margin) + jax.nn.log_sigmoid(forget_projected.astype(jnp.float32)),
    )
    key_gate_values = -jnp.expm1(log_forget_gate)
    log_decay_running = (
        log_forget_gate.reshape(row_total_count, head_total_count, -1) + decay_jump_rows[:, :, None]
    )
    return (
        query_rows.reshape(row_total_count, head_total_count, -1),
        key_gate_values.reshape(row_total_count, head_total_count, -1),
        log_decay_running,
    )


def finish(recurrent, gain, outgate_proj):
    row_total_count = recurrent.shape[0]
    scaled = recurrent * lax.rsqrt(
        jnp.mean(recurrent * recurrent, axis=2, keepdims=True) + norm_eps
    )
    gated_out = (
        scaled.reshape(row_total_count, -1) * gain * jax.nn.silu(outgate_proj.astype(jnp.float32))
    )
    return gated_out.astype(jnp.bfloat16)


def combine_states(first_part, second_part):
    return (
        first_part[0] + second_part[0],
        jnp.exp(second_part[0])[:, :, None] * first_part[1] + second_part[1],
    )


def carry_step(recurrence_state, block_parts):
    decay_end, contribution = block_parts
    return (jnp.exp(decay_end)[:, :, None] * recurrence_state + contribution, recurrence_state)


def per_device(
    tokens,
    input_norm_gain,
    convolution_value_weight,
    convolution_gate_weight,
    depthwise_filter_taps,
    channel_norm_gain,
    channel_norm_bias,
    query_projection_weight,
    forget_gate_weight,
    recurrence_value_weight,
    output_gate_weight,
    forget_floor_margin,
    decay_jump_terms,
    head_norm_gain,
    convolution_output_weight,
    recurrence_output_weight,
):
    features = tokens.astype(jnp.float32)
    normed = (
        features
        * lax.rsqrt(jnp.mean(features * features, axis=1, keepdims=True) + norm_eps)
        * input_norm_gain
    ).astype(jnp.bfloat16)
    gathered = (
        lax.all_gather(convolution_value_weight, "sp", axis=0, tiled=True),
        lax.all_gather(convolution_gate_weight, "sp", axis=0, tiled=True),
        lax.all_gather(query_projection_weight, "sp", axis=0, tiled=True),
        lax.all_gather(forget_gate_weight, "sp", axis=0, tiled=True),
        lax.all_gather(recurrence_value_weight, "sp", axis=0, tiled=True),
        lax.all_gather(output_gate_weight, "sp", axis=0, tiled=True),
        lax.all_gather(convolution_output_weight, "sp", axis=1, tiled=True),
        lax.all_gather(recurrence_output_weight, "sp", axis=1, tiled=True),
    )
    projection_weights = gathered[:6]
    conv_columns = gathered[6]
    rec_columns = gathered[7]

    def project(row_piece):
        return jnp.concatenate(
            [
                jnp.dot(row_piece, weight, preferred_element_type=jnp.float32).astype(jnp.bfloat16)
                for weight in projection_weights
            ],
            axis=1,
        )

    projected = project(lax.all_gather(normed, "tp", axis=0, tiled=True))
    offsets = []
    position = 0
    for weight in projection_weights[:-1]:
        position = position + weight.shape[1]
        offsets.append(position)
    value_proj, gate_proj, query_projected, forget_projected, input_proj, outgate_proj = jnp.split(
        projected, offsets, axis=1
    )
    row_total_count = value_proj.shape[0]
    rim_rows = depthwise_filter_taps.shape[0] - 1
    tail_value, tail_gate = passed_along(
        (value_proj[row_total_count - rim_rows :], gate_proj[row_total_count - rim_rows :]), "sp", 1
    )
    value_ext = jnp.concatenate([tail_value, value_proj], axis=0)
    gate_ext = jnp.concatenate([tail_gate, gate_proj], axis=0)
    gated = value_ext.astype(jnp.float32) * jax.nn.sigmoid(gate_ext.astype(jnp.float32))
    convolved = convolve(gated, depthwise_filter_taps).astype(jnp.bfloat16)
    device_heads = decay_jump_terms.shape[0]
    query_rows, key_gate_values, log_decay_running = gate_factors(
        query_projected, forget_projected, forget_floor_margin, decay_jump_terms.T
    )
    input_rows = input_proj.astype(jnp.float32).reshape(row_total_count, device_heads, -1)
    block_count = row_total_count // HG_BLOCK

    def to_blocks(array):
        return array.reshape(block_count, HG_BLOCK, device_heads, -1).transpose(0, 2, 1, 3)

    block_queries = to_blocks(query_rows)
    block_keys = to_blocks(key_gate_values)
    block_inputs = to_blocks(input_rows)
    cumulative = jnp.cumsum(to_blocks(log_decay_running), axis=2)
    final_decay = cumulative[:, :, -1, :]
    query_rows_scaled = block_queries * jnp.exp(cumulative)
    scaled_keys = block_keys * jnp.exp(-cumulative)
    final_keys = block_keys * jnp.exp(final_decay[:, :, None, :] - cumulative)
    attention_scores = jnp.einsum(
        "nhtk,nhsk->nhts", query_rows_scaled, scaled_keys, precision=highest_precision
    )
    causal = jnp.arange(HG_BLOCK)[:, None] >= jnp.arange(HG_BLOCK)[None, :]
    attention_scores = jnp.where(causal[None, None], attention_scores, 0.0)
    inner = jnp.einsum(
        "nhts,nhsv->nhtv", attention_scores, block_inputs, precision=highest_precision
    )
    contributions = jnp.einsum(
        "nhsk,nhsv->nhkv", final_keys, block_inputs, precision=highest_precision
    )
    initial = jnp.zeros((device_heads, HG_DK, HG_DV), jnp.float32)
    local_state, block_starts = lax.scan(carry_step, initial, (final_decay, contributions))
    device_decay = jnp.sum(final_decay, axis=0)
    before_blocks = jnp.cumsum(final_decay, axis=0) - final_decay
    incoming = prefix(
        (device_decay, local_state),
        "sp",
        combine_states,
        (jnp.zeros_like(device_decay), jnp.zeros_like(local_state)),
    )
    starts = block_starts + jnp.exp(before_blocks)[:, :, :, None] * incoming[1][None]
    recurrent = inner + jnp.einsum(
        "nhtk,nhkv->nhtv", query_rows_scaled, starts, precision=highest_precision
    )
    recurrent = recurrent.transpose(0, 2, 1, 3).reshape(row_total_count, device_heads, -1)
    rec_out = finish(recurrent, head_norm_gain, outgate_proj)
    values = convolved.astype(jnp.float32)
    totals = lax.psum((jnp.sum(values, axis=1), jnp.sum(values * values, axis=1)), "tp")
    conv_out = channel_norm(values, totals[0], totals[1], channel_norm_gain, channel_norm_bias)
    conv_part = lax.slice_in_dim(
        conv_out, 0, row_total_count // lax.axis_size("tp") * lax.axis_size("tp"), axis=0
    )
    return lax.psum_scatter(
        (
            jnp.dot(conv_part, conv_columns, preferred_element_type=jnp.float32)
            + jnp.dot(rec_out, rec_columns, preferred_element_type=jnp.float32)
        ).astype(jnp.bfloat16),
        "tp",
        scatter_dimension=0,
        tiled=True,
    )


MESH = pl.DeviceIdType.MESH
STRIDE = 2
NT = (((1,), (1,)), ((), ()))
TN = (((0,), (0,)), ((), ()))


def at(sp, tp):
    return {"sp": sp, "tp": tp}


def greet(peers):
    barrier = pltpu.get_barrier_semaphore()
    for peer in peers:
        pl.semaphore_signal(barrier, inc=1, device_id=peer, device_id_type=MESH)
    pl.semaphore_wait(barrier, len(peers))


def remote(src, dst, send, recv, peer):
    return pltpu.make_async_remote_copy(
        src_ref=src, dst_ref=dst, send_sem=send, recv_sem=recv, device_id=peer, device_id_type=MESH
    )


def project_kernel(
    sizes, x_hbm, gain_ref, j_ref, cv, cg, rv, og, qw, fw, co, ro, p_ref, qf_ref, jump_ref, wo_ref,
    x_ref, raw, w_ref, held, weights, load, *sems
):
    n_sp, n_tp, rows, depth, chans, members = sizes
    (send_z, send_x, send_y, send_c, lane, sib, send_w, recv_w, send_j, recv_j, send_q, recv_q, swap) = sems
    s, t = lax.axis_index("sp"), lax.axis_index("tp")
    n_z = n_sp // STRIDE
    z, x = s // STRIDE, s % STRIDE
    y, c = t // 2, t % 2
    x_peer = at(z * STRIDE + (1 - x), t)
    y_peer = at(s, (1 - y) * 2 + c)
    c_peer = at(s, y * 2 + (1 - c))
    total = held.shape[0]
    half = total // 2

    def sp_peer(k):
        return lax.rem(s + k, n_sp)

    def slot(dy, dx, dz, core):
        from_z = lax.rem(z - dz + n_z, n_z)
        from_x = (1 - x) if dx else x
        from_y = (1 - y) if dy else y
        start = from_y * half + ((from_z * STRIDE + from_x) * 2 + core) * rows
        return pl.ds(pl.multiple_of(start, rows), rows)

    def number(dy, dx, dz):
        return (dy * STRIDE + dx) * n_z + dz

    peers = [at(sp_peer(k), t) for k in range(1, n_sp)] + [y_peer, c_peer]
    barrier = pltpu.get_barrier_semaphore()
    for peer in peers:
        pl.semaphore_signal(barrier, inc=1, device_id=peer, device_id_type=MESH)
    kinds = (cv, cg, rv, og, qw, fw)
    loads = [pltpu.make_async_copy(x_hbm, x_ref, load.at[0])] + [
        pltpu.make_async_copy(w, raw.at[i], load.at[1 + i]) for i, w in enumerate(kinds)
    ]
    cols = co.shape[1]
    swapped = wo_ref.at[:, pl.ds(pl.multiple_of(z % 2 * cols, cols), cols)]
    for i, w in enumerate((co, ro)):
        tall = w.shape[0]
        loads.append(pltpu.make_async_copy(w, swapped.at[i * tall : (i + 1) * tall, :], load.at[1 + len(kinds) + i]))
    for copy in loads:
        copy.start()
    own = slot(0, 0, 0, c)
    mine = held.at[own]
    loads[0].wait()
    features = x_ref[...].astype(jnp.float32)
    mine[...] = (
        features
        * lax.rsqrt(jnp.mean(features * features, axis=1, keepdims=True) + norm_eps)
        * gain_ref[...]
    ).astype(jnp.bfloat16)
    pl.semaphore_wait(barrier, len(peers))
    pending = []

    def launch(copy):
        copy.start()
        pending.append(copy)

    def pass_on(dy, dx, dz):
        here = held.at[slot(dy, dx, dz, c)]
        at_number = number(dy, dx, dz)
        if not dy:
            if not dx:
                launch(remote(here, here, send_x.at[dz], lane.at[number(0, 1, dz)], x_peer))
            launch(remote(here, here, send_y.at[at_number], lane.at[number(1, dx, dz)], y_peer))
        launch(remote(here, here, send_c.at[at_number], sib.at[at_number], c_peer))

    near_first = sorted(range(1, n_z), key=lambda k: min(k, n_z - k))
    for k in near_first:
        peer = at(lax.rem(z + k, n_z) * STRIDE + x, t)
        launch(remote(mine, mine, send_z.at[k], lane.at[k], peer))
    pass_on(0, 0, 0)
    for k in range(1, n_sp):
        launch(remote(j_ref, jump_ref.at[s], send_j.at[k], recv_j.at[k], at(sp_peer(k), t)))
    jump_ref[s] = j_ref[...]
    for i in range(len(kinds)):
        loads[1 + i].wait()
        turned = raw[i].T
        for d in range(n_sp):
            w_ref[d, i * chans : (i + 1) * chans, :] = turned[d * chans : (d + 1) * chans]
    my_columns = pl.ds(pl.multiple_of(s * depth, depth), depth)

    def send_weights(dx, dz):
        other = lax.rem(z + dz, n_z) * STRIDE + ((1 - x) if dx else x)
        k = dx * n_z + dz
        launch(remote(w_ref.at[other], weights.at[:, my_columns], send_w.at[k], recv_w.at[k], at(other, t)))

    for dz in near_first:
        send_weights(0, dz)
    weights[:, my_columns] = w_ref[s]
    for copy in loads[1 + len(kinds) :]:
        copy.wait()
    partner = at((z + 1 - z % 2 * 2) * STRIDE + x, t)
    launch(remote(swapped, swapped, swap.at[0], swap.at[1], partner))

    def arrived(dy, dx, dz):
        here = held.at[slot(dy, dx, dz, c)]
        remote(here, here, send_c.at[0], lane.at[number(dy, dx, dz)], c_peer).wait_recv()
        pass_on(dy, dx, dz)

    order = []
    for dz in near_first:
        order += [(0, dz), (1, 0 if dz == near_first[0] else order[-2][1])]
    order.append((1, near_first[-1]))
    for dx, dz in order:
        arrived(0, dx, dz)
    for dz in [0] + near_first:
        send_weights(1, dz)
    across = [(0, 0)] + order
    early = len(across) // 2 + 1
    for dx, dz in across[:early]:
        arrived(1, dx, dz)
    for dx in range(STRIDE):
        for dz in range(n_z):
            if dx or dz:
                source = lax.rem(z - dz + n_z, n_z) * STRIDE + ((1 - x) if dx else x)
                there = weights.at[:, pl.ds(pl.multiple_of(source * depth, depth), depth)]
                k = dx * n_z + dz
                remote(there, there, send_w.at[k], recv_w.at[k], c_peer).wait_recv()
    member = lax.rem(s, members)
    first = s - member

    def project_half(dy):
        for dx in range(STRIDE):
            for dz in range(n_z):
                here = held.at[slot(dy, dx, dz, 1 - c)]
                remote(here, here, send_c.at[0], sib.at[number(dy, dx, dz)], c_peer).wait_recv()
        base = ((1 - y) if dy else y) * half
        step = min(256, half)
        for start in range(0, half, step):
            span = pl.ds(pl.multiple_of(base + start, step), step)
            piece = lax.dot_general(
                held[span, :], weights[...], NT, preferred_element_type=jnp.float32
            ).T.astype(jnp.bfloat16)
            qf_ref[member, :, span] = piece[4 * chans :]
            p_ref[:, span] = piece[: 4 * chans]
        window = pl.ds(pl.multiple_of(base, half), half)
        for k in range(1, members):
            peer = at(first + lax.rem(member + k, members), t)
            block = qf_ref.at[member, :, window]
            launch(remote(block, block, send_q.at[dy, k], recv_q.at[dy, k], peer))

    project_half(0)
    for dx, dz in across[early:]:
        arrived(1, dx, dz)
    project_half(1)
    for dy in range(2):
        window = pl.ds(pl.multiple_of(((1 - y) if dy else y) * half, half), half)
        for k in range(1, members):
            there = qf_ref.at[lax.rem(member - k + members, members), :, window]
            remote(there, there, send_q.at[dy, k], recv_q.at[dy, k], c_peer).wait_recv()
    for k in range(1, n_sp):
        there = jump_ref.at[lax.rem(s - k + n_sp, n_sp)]
        remote(there, there, send_j.at[k], recv_j.at[k], c_peer).wait_recv()
    other = wo_ref.at[:, pl.ds(pl.multiple_of((1 - z % 2) * cols, cols), cols)]
    remote(other, other, swap.at[0], swap.at[1], c_peer).wait_recv()
    for copy in pending:
        copy.wait_send()


def in_order(array, n_sp):
    half = array.shape[1] // 2
    own = half // n_sp
    return jnp.concatenate(
        [
            array[:, side * half + b * own : side * half + (b + 1) * own]
            for b in range(n_sp)
            for side in range(2)
        ],
        axis=1,
    )


def mix_kernel(sizes, p_ref, qf_ref, jump_ref, par_ref, a_ref, q_s, k_s, d_s, r_s):
    n_sp, chans, members, width, block, part = sizes
    s = lax.axis_index("sp")
    total = p_ref.shape[1]
    f32, bf16 = jnp.float32, jnp.bfloat16
    mine = par_ref[pl.ds(pl.multiple_of(s * chans, chans), chans), :]
    head = s // members
    span = chans * members
    margin = par_ref[pl.ds(pl.multiple_of(head * span, span), span), width + 1 : width + 2]

    projected = in_order(p_ref[...].astype(f32), n_sp)
    value = projected[0:chans]
    gate = projected[chans : 2 * chans]
    gated = value * jax.nn.sigmoid(gate)
    place = lax.broadcasted_iota(jnp.int32, gated.shape, 1)
    conv = gated * mine[:, width - 1 : width]
    for back in range(1, width):
        moved = jnp.where(place >= back, pltpu.roll(gated, back, 1), 0.0)
        conv = conv + moved * mine[:, width - 1 - back : width - back]

    def put(start, stop, array):
        for b in range(n_sp):
            place = (b // (2 * STRIDE)) * STRIDE + b % STRIDE
            a_ref[(b // STRIDE) % 2, start:stop, place * part : (place + 1) * part] = array[
                :, b * part : (b + 1) * part
            ]

    put(0, chans, conv.astype(bf16))

    picked = lax.broadcasted_iota(jnp.int32, jump_ref.shape[1:], 0) == head
    arranged = [in_order(qf_ref[m].astype(f32), n_sp) for m in range(members)]
    for b in range(n_sp):
        lanes = slice(b * part, (b + 1) * part)
        jump = jnp.sum(jnp.where(picked, jump_ref[b], 0.0), axis=0, keepdims=True)
        both = [arranged[m][:, lanes] for m in range(members)]
        query = jnp.concatenate([v[:chans] for v in both], axis=0)
        forget = jnp.concatenate([v[chans:] for v in both], axis=0)
        key = margin * jax.nn.sigmoid(-forget)
        q_s[lanes, :] = (query * jax.nn.sigmoid(query)).T
        k_s[lanes, :] = key.T
        d_s[lanes, :] = (jnp.log1p(-key) + jump).T
    low = lax.broadcasted_iota(jnp.int32, (block, block), 0) >= lax.broadcasted_iota(
        jnp.int32, (block, block), 1
    )
    tri = low.astype(bf16)
    inputs = projected[2 * chans : 3 * chans].T.astype(bf16)
    state = jnp.zeros((span, chans), f32)
    for n in range(total // block):
        at_rows = slice(n * block, (n + 1) * block)
        decay = d_s[at_rows, :]
        high = decay.astype(bf16)
        rest = (decay - high.astype(f32)).astype(bf16)
        cum = jnp.dot(tri, high, preferred_element_type=f32) + jnp.dot(
            tri, rest, preferred_element_type=f32
        )
        last = cum[block - 1 : block, :]
        qs = (q_s[at_rows, :] * jnp.exp(cum)).astype(bf16)
        key = k_s[at_rows, :]
        ks = (key * jnp.exp(-cum)).astype(bf16)
        kf = (key * jnp.exp(last - cum)).astype(bf16)
        rows_in = inputs[at_rows, :]
        scores = lax.dot_general(qs, ks, NT, preferred_element_type=f32)
        scores = jnp.where(low, scores, 0.0).astype(bf16)
        r_s[at_rows, :] = jnp.dot(scores, rows_in, preferred_element_type=f32) + jnp.dot(
            qs, state.astype(bf16), preferred_element_type=f32
        )
        state = jnp.exp(last).T * state + lax.dot_general(
            kf, rows_in, TN, preferred_element_type=f32
        )
    rec = r_s[...].T
    outgate = projected[3 * chans : 4 * chans]
    square = jnp.sum(rec * rec, axis=0, keepdims=True)
    put(
        chans,
        2 * chans,
        (rec * mine[:, width : width + 1] * (outgate * jax.nn.sigmoid(outgate))).astype(bf16),
    )
    upper = square.astype(bf16).astype(f32)
    tall = a_ref.shape[1]
    line = lax.broadcasted_iota(jnp.int32, (tall - 2 * chans, total), 0)
    put(
        2 * chans,
        tall,
        jnp.where(line == 0, upper, jnp.where(line == 1, square - upper, 0.0)).astype(bf16),
    )


def output_kernel(
    sizes, a_ref, wo_ref, par_ref, o_ref, held, sums, part, got, mixed, *sems
):
    n_sp, n_tp, rows, chans, members, width, channels = sizes
    send_z, send_x, recv_z, recv_x, send_s, recv_s, send_p, recv_p, send_o, recv_o = sems
    f32, bf16 = jnp.float32, jnp.bfloat16
    s, t = lax.axis_index("sp"), lax.axis_index("tp")
    n_z = n_sp // STRIDE
    z, x = s // STRIDE, s % STRIDE
    parity = z % 2
    x_peer = at(z * STRIDE + (1 - x), t)

    def sp_at(k):
        return lax.rem(s + k, n_sp)

    def tp_at(k):
        return lax.rem(t + k, n_tp)

    greet([at(sp_at(k), t) for k in range(1, n_sp)] + [at(s, tp_at(k)) for k in range(1, n_tp)])
    pending = []

    def launch(copy):
        copy.start()
        pending.append(copy)

    near_first = sorted(range(1, n_z), key=lambda k: min(k, n_z - k))
    for k in near_first:
        z_to = lax.rem(z + k, n_z)
        launch(
            remote(a_ref.at[z_to % 2], held.at[s], send_z.at[k], recv_z.at[k], at(z_to * STRIDE + x, t))
        )
    launch(remote(a_ref.at[parity], held.at[s], send_x.at[0], recv_x.at[0], x_peer))
    held[s] = a_ref[parity]
    for k in near_first:
        here = held.at[lax.rem(z - k + n_z, n_z) * STRIDE + x]
        remote(here, here, send_z.at[k], recv_z.at[k], x_peer).wait_recv()
        launch(remote(here, here, send_x.at[k], recv_x.at[k], x_peer))
    for k in [0] + near_first:
        here = held.at[lax.rem(z - k + n_z, n_z) * STRIDE + (1 - x)]
        remote(here, here, send_x.at[k], recv_x.at[k], x_peer).wait_recv()

    total = a_ref.shape[2]
    conv = held[:, 0:chans, :].reshape(n_sp * chans, total).astype(f32)
    sums[t, 0:1, :] = jnp.sum(conv, axis=0, keepdims=True)
    sums[t, 1:2, :] = jnp.sum(conv * conv, axis=0, keepdims=True)
    for k in range(1, n_tp):
        launch(remote(sums.at[t], sums.at[t], send_s.at[k], recv_s.at[k], at(s, tp_at(k))))
    for k in range(1, n_tp):
        there = sums.at[lax.rem(t - k + n_tp, n_tp)]
        remote(there, there, send_s.at[k], recv_s.at[k], x_peer).wait_recv()
    both = sums[0]
    for k in range(1, n_tp):
        both = both + sums[k]
    sums[n_tp] = both
    gain = par_ref[:, width + 2 : width + 3]
    bias = par_ref[:, width + 3 : width + 4]
    span = members * chans
    heads = n_sp // members
    step = rows * n_tp
    blocks = n_sp // 2
    here = (z // 2) * STRIDE + x

    def device(place):
        return (place // STRIDE * 2 + parity) * STRIDE + place % STRIDE

    def project_block(r):
        lanes = pl.ds(pl.multiple_of(lax.rem(here + r, blocks) * step, step), step)
        mean = sums[n_tp, 0:1, lanes] / channels
        scale = lax.rsqrt(sums[n_tp, 1:2, lanes] / channels - mean * mean + layer_eps)
        values = held[:, 0:chans, lanes].reshape(n_sp * chans, step).astype(f32)
        shifted = (values - mean) * scale * gain + bias
        pieces = [(shifted * jax.nn.sigmoid(shifted)).astype(bf16)]
        for h in range(heads):
            group = slice(h * members, (h + 1) * members)
            square = jnp.sum(
                held[group, 2 * chans : 2 * chans + 16, lanes].astype(f32), axis=(0, 1), keepdims=True
            )[0]
            ups = held[group, chans : 2 * chans, lanes].reshape(span, step).astype(f32)
            pieces.append((ups * lax.rsqrt(square / span + norm_eps)).astype(bf16))
        out = lax.dot_general(
            jnp.concatenate(pieces, axis=0), wo_ref[...], TN, preferred_element_type=f32
        ).astype(bf16)
        for k in range(n_tp):
            part[k, r] = out[k * rows : (k + 1) * rows]
        for k in range(1, n_tp):
            launch(
                remote(part.at[tp_at(k), r], got.at[k, r], send_p.at[k, r], recv_p.at[k, r], at(s, tp_at(k)))
            )

    cols = wo_ref.shape[1] // 2

    def window(place, p):
        column = (place // STRIDE * 2 + p) * STRIDE + place % STRIDE
        return o_ref.at[:, pl.ds(pl.multiple_of(column * cols, cols), cols)]

    def finish_block(r):
        added = part[t, r].astype(f32)
        for k in range(1, n_tp):
            remote(got.at[k, r], got.at[k, r], send_p.at[k, r], recv_p.at[k, r], x_peer).wait_recv()
            added = added + got[k, r].astype(f32)
        mixed[r] = added.astype(bf16)
        for p in range(2):
            piece = mixed.at[r, :, p * cols : (p + 1) * cols]
            if r:
                to = at(device(lax.rem(here + r, blocks)), t)
                launch(remote(piece, window(here, p), send_o.at[r, p], recv_o.at[r, p], to))
            else:
                window(here, p)[...] = piece[...]

    order = list(range(1, blocks)) + [0]
    for r in order:
        project_block(r)
    for r in order:
        finish_block(r)
    for r in range(1, blocks):
        for p in range(2):
            there = window(lax.rem(here - r + blocks, blocks), p)
            remote(there, there, send_o.at[r, p], recv_o.at[r, p], x_peer).wait_recv()
    for copy in pending:
        copy.wait_send()


def spread_channels(n_sp, n_tp,
    tokens,
    input_norm_gain,
    convolution_value_weight,
    convolution_gate_weight,
    depthwise_filter_taps,
    channel_norm_gain,
    channel_norm_bias,
    query_projection_weight,
    forget_gate_weight,
    recurrence_value_weight,
    output_gate_weight,
    forget_floor_margin,
    decay_jump_terms,
    head_norm_gain,
    convolution_output_weight,
    recurrence_output_weight,
):
    rows, model = tokens.shape
    total = rows * n_sp * n_tp
    depth, group_chans = convolution_value_weight.shape
    chans = group_chans // n_sp
    heads, part = decay_jump_terms.shape
    members = n_sp // heads
    width = depthwise_filter_taps.shape[0]
    kinds = (
        convolution_value_weight,
        convolution_gate_weight,
        recurrence_value_weight,
        output_gate_weight,
        query_projection_weight,
        forget_gate_weight,
    )
    jumps = jnp.pad(decay_jump_terms, ((0, -heads % 8), (0, 0)))
    params = jnp.concatenate(
        [
            depthwise_filter_taps.T,
            head_norm_gain[:, None],
            forget_floor_margin[:, None],
            channel_norm_gain[:, None],
            channel_norm_bias[:, None],
        ],
        axis=1,
    )
    cols = convolution_output_weight.shape[1]
    vmem = pl.BlockSpec(memory_space=pltpu.VMEM)
    anywhere = pl.BlockSpec(memory_space=pl.ANY)
    dma = pltpu.SemaphoreType.DMA
    bf16, f32 = jnp.bfloat16, jnp.float32
    n_z = n_sp // STRIDE
    lanes = 2 * n_sp
    projected, query_forget, all_jumps, weights_out = pl.pallas_call(
        functools.partial(project_kernel, (n_sp, n_tp, rows, depth, chans, members)),
        out_shape=(
            jax.ShapeDtypeStruct((4 * chans, total), bf16),
            jax.ShapeDtypeStruct((members, 2 * chans, total), bf16),
            jax.ShapeDtypeStruct((n_sp, *jumps.shape), f32),
            jax.ShapeDtypeStruct((2 * group_chans, 2 * cols), bf16),
        ),
        in_specs=[anywhere, vmem, vmem] + [anywhere] * (len(kinds) + 2),
        out_specs=(vmem,) * 4,
        scratch_shapes=[
            pltpu.VMEM((rows, model), bf16),
            pltpu.VMEM((len(kinds), depth, group_chans), bf16),
            pltpu.VMEM((n_sp, len(kinds) * chans, depth), bf16),
            pltpu.VMEM((total, model), bf16),
            pltpu.VMEM((len(kinds) * chans, model), bf16),
            dma((3 + len(kinds),)),
            dma((n_z,)),
            dma((n_z,)),
            dma((lanes,)),
            dma((lanes,)),
            dma((lanes,)),
            dma((lanes,)),
            dma((n_sp,)),
            dma((n_sp,)),
            dma((n_sp,)),
            dma((n_sp,)),
            dma((2, members)),
            dma((2, members)),
            dma((2,)),
        ],
        compiler_params=pltpu.CompilerParams(collective_id=0, has_side_effects=True),
        name="project",
    )(
        tokens,
        input_norm_gain[None, :],
        jumps,
        *kinds,
        convolution_output_weight,
        recurrence_output_weight,
    )
    span = members * chans
    sent = pl.pallas_call(
        functools.partial(mix_kernel, (n_sp, chans, members, width, HG_BLOCK, part)),
        out_shape=jax.ShapeDtypeStruct((2, 2 * chans + 16, total // 2), bf16),
        in_specs=[vmem] * 4,
        out_specs=vmem,
        scratch_shapes=[pltpu.VMEM((total, span), f32)] * 3 + [pltpu.VMEM((total, chans), f32)],
        name="mix",
    )(projected, query_forget, all_jumps, params)
    return pl.pallas_call(
        functools.partial(
            output_kernel, (n_sp, n_tp, rows, chans, members, width, group_chans * n_tp)
        ),
        out_shape=jax.ShapeDtypeStruct((rows, model), bf16),
        in_specs=[vmem] * 3,
        out_specs=vmem,
        scratch_shapes=[
            pltpu.VMEM((n_sp, 2 * chans + 16, total // 2), bf16),
            pltpu.VMEM((n_tp + 1, 8, total // 2), f32),
            pltpu.VMEM((n_tp, n_sp // 2, rows, 2 * cols), bf16),
            pltpu.VMEM((n_tp, n_sp // 2, rows, 2 * cols), bf16),
            pltpu.VMEM((n_sp // 2, rows, 2 * cols), bf16),
            dma((n_z,)),
            dma((n_z,)),
            dma((n_z,)),
            dma((n_z,)),
            dma((n_tp,)),
            dma((n_tp,)),
            dma((n_tp, n_sp // 2)),
            dma((n_tp, n_sp // 2)),
            dma((n_sp // 2, 2)),
            dma((n_sp // 2, 2)),
        ],
        compiler_params=pltpu.CompilerParams(collective_id=1, has_side_effects=True),
        name="output",
    )(sent, weights_out, params)


def layer(n_sp, n_tp, *arrays):
    rows, model = arrays[0].shape
    group_chans = arrays[2].shape[1]
    heads = arrays[12].shape[0]
    gathered_bytes = rows * n_sp * n_tp * model * arrays[0].dtype.itemsize
    fits = gathered_bytes <= 2**23
    even = n_tp == 4 and n_sp % heads == 0 and n_sp % (2 * STRIDE) == 0 and group_chans % (32 * n_sp) == 0
    if fits and even:
        return spread_channels(n_sp, n_tp, *arrays)
    return per_device(*arrays)


def solution(mesh):
    in_specs = (
        P(("sp", "tp"), None),
        P(),
        P("sp", "tp"),
        P("sp", "tp"),
        P(None, "tp"),
        P("tp"),
        P("tp"),
        P("sp", "tp"),
        P("sp", "tp"),
        P("sp", "tp"),
        P("sp", "tp"),
        P("tp"),
        P("tp", "sp"),
        P("tp"),
        P("tp", "sp"),
        P("tp", "sp"),
    )
    out_specs = P(("sp", "tp"), None)
    return jax.shard_map(
        functools.partial(layer, mesh.shape["sp"], mesh.shape["tp"]), mesh=mesh, in_specs=in_specs, out_specs=out_specs, check_vma=False
    )
```

```python
import functools

import jax
import jax.numpy as jnp
from jax import lax
from jax.experimental import pallas as pl
from jax.experimental.pallas import tpu as pltpu
from jax.sharding import PartitionSpec as P

CONV_CH = 1024
HG_DK = 128
HG_DV = 128
HG_BLOCK = 64


norm_eps = 1e-06
layer_eps = 1e-05
highest_precision = lax.Precision.HIGHEST


def passed_along(value, axis, steps):
    count = lax.axis_size(axis)
    initial, last = (max(0, -steps), min(count, count - steps))
    return lax.ppermute(value, axis, [(source, source + steps) for source in range(initial, last)])


def prefix(x, axis, combine, identity):
    size, mine = (lax.axis_size(axis), lax.axis_index(axis))
    everything = jax.tree.map(
        lambda part, kind: lax.all_gather(part.astype(kind), axis), x, (jnp.bfloat16, jnp.bfloat16)
    )
    start = jax.tree.map(
        lambda part, zero: jnp.broadcast_to(jnp.asarray(zero, part.dtype), part.shape), x, identity
    )

    def lap(k, before):
        reached = k < mine
        new = combine(
            before, jax.tree.map(lambda part, own: part[k].astype(own.dtype), everything, x)
        )
        return jax.tree.map(lambda a, b: jnp.where(reached, a, b), new, before)

    return lax.fori_loop(0, size, lap, start)


def convolve(gated, kernel):
    return lax.conv_general_dilated(
        gated[None],
        kernel[:, None, :],
        (1,),
        "VALID",
        dimension_numbers=("NWC", "WIO", "NWC"),
        feature_group_count=gated.shape[1],
        precision=highest_precision,
    )[0]


def channel_norm(values, first_sum, second_sum, gain, bias):
    mean_value = first_sum[:, None] / CONV_CH
    variance = second_sum[:, None] / CONV_CH - mean_value * mean_value
    shifted = (values - mean_value) * lax.rsqrt(variance + layer_eps) * gain + bias
    return jax.nn.silu(shifted).astype(jnp.bfloat16)


def gate_factors(query_projected, forget_projected, forget_floor_margin, decay_jump_rows):
    row_total_count = query_projected.shape[0]
    head_total_count = decay_jump_rows.shape[1]
    query_rows = jax.nn.silu(query_projected.astype(jnp.float32))
    log_forget_gate = jnp.logaddexp(
        jnp.log1p(-forget_floor_margin),
        jnp.log(forget_floor_margin) + jax.nn.log_sigmoid(forget_projected.astype(jnp.float32)),
    )
    key_gate_values = -jnp.expm1(log_forget_gate)
    log_decay_running = (
        log_forget_gate.reshape(row_total_count, head_total_count, -1) + decay_jump_rows[:, :, None]
    )
    return (
        query_rows.reshape(row_total_count, head_total_count, -1),
        key_gate_values.reshape(row_total_count, head_total_count, -1),
        log_decay_running,
    )


def finish(recurrent, gain, outgate_proj):
    row_total_count = recurrent.shape[0]
    scaled = recurrent * lax.rsqrt(
        jnp.mean(recurrent * recurrent, axis=2, keepdims=True) + norm_eps
    )
    gated_out = (
        scaled.reshape(row_total_count, -1) * gain * jax.nn.silu(outgate_proj.astype(jnp.float32))
    )
    return gated_out.astype(jnp.bfloat16)


def combine_states(first_part, second_part):
    return (
        first_part[0] + second_part[0],
        jnp.exp(second_part[0])[:, :, None] * first_part[1] + second_part[1],
    )


def carry_step(recurrence_state, block_parts):
    decay_end, contribution = block_parts
    return (jnp.exp(decay_end)[:, :, None] * recurrence_state + contribution, recurrence_state)


def per_device(
    tokens,
    input_norm_gain,
    convolution_value_weight,
    convolution_gate_weight,
    depthwise_filter_taps,
    channel_norm_gain,
    channel_norm_bias,
    query_projection_weight,
    forget_gate_weight,
    recurrence_value_weight,
    output_gate_weight,
    forget_floor_margin,
    decay_jump_terms,
    head_norm_gain,
    convolution_output_weight,
    recurrence_output_weight,
):
    features = tokens.astype(jnp.float32)
    normed = (
        features
        * lax.rsqrt(jnp.mean(features * features, axis=1, keepdims=True) + norm_eps)
        * input_norm_gain
    ).astype(jnp.bfloat16)
    gathered = (
        lax.all_gather(convolution_value_weight, "sp", axis=0, tiled=True),
        lax.all_gather(convolution_gate_weight, "sp", axis=0, tiled=True),
        lax.all_gather(query_projection_weight, "sp", axis=0, tiled=True),
        lax.all_gather(forget_gate_weight, "sp", axis=0, tiled=True),
        lax.all_gather(recurrence_value_weight, "sp", axis=0, tiled=True),
        lax.all_gather(output_gate_weight, "sp", axis=0, tiled=True),
        lax.all_gather(convolution_output_weight, "sp", axis=1, tiled=True),
        lax.all_gather(recurrence_output_weight, "sp", axis=1, tiled=True),
    )
    projection_weights = gathered[:6]
    conv_columns = gathered[6]
    rec_columns = gathered[7]

    def project(row_piece):
        return jnp.concatenate(
            [
                jnp.dot(row_piece, weight, preferred_element_type=jnp.float32).astype(jnp.bfloat16)
                for weight in projection_weights
            ],
            axis=1,
        )

    projected = project(lax.all_gather(normed, "tp", axis=0, tiled=True))
    offsets = []
    position = 0
    for weight in projection_weights[:-1]:
        position = position + weight.shape[1]
        offsets.append(position)
    value_proj, gate_proj, query_projected, forget_projected, input_proj, outgate_proj = jnp.split(
        projected, offsets, axis=1
    )
    row_total_count = value_proj.shape[0]
    rim_rows = depthwise_filter_taps.shape[0] - 1
    tail_value, tail_gate = passed_along(
        (value_proj[row_total_count - rim_rows :], gate_proj[row_total_count - rim_rows :]), "sp", 1
    )
    value_ext = jnp.concatenate([tail_value, value_proj], axis=0)
    gate_ext = jnp.concatenate([tail_gate, gate_proj], axis=0)
    gated = value_ext.astype(jnp.float32) * jax.nn.sigmoid(gate_ext.astype(jnp.float32))
    convolved = convolve(gated, depthwise_filter_taps).astype(jnp.bfloat16)
    device_heads = decay_jump_terms.shape[0]
    query_rows, key_gate_values, log_decay_running = gate_factors(
        query_projected, forget_projected, forget_floor_margin, decay_jump_terms.T
    )
    input_rows = input_proj.astype(jnp.float32).reshape(row_total_count, device_heads, -1)
    block_count = row_total_count // HG_BLOCK

    def to_blocks(array):
        return array.reshape(block_count, HG_BLOCK, device_heads, -1).transpose(0, 2, 1, 3)

    block_queries = to_blocks(query_rows)
    block_keys = to_blocks(key_gate_values)
    block_inputs = to_blocks(input_rows)
    cumulative = jnp.cumsum(to_blocks(log_decay_running), axis=2)
    final_decay = cumulative[:, :, -1, :]
    query_rows_scaled = block_queries * jnp.exp(cumulative)
    scaled_keys = block_keys * jnp.exp(-cumulative)
    final_keys = block_keys * jnp.exp(final_decay[:, :, None, :] - cumulative)
    attention_scores = jnp.einsum(
        "nhtk,nhsk->nhts", query_rows_scaled, scaled_keys, precision=highest_precision
    )
    causal = jnp.arange(HG_BLOCK)[:, None] >= jnp.arange(HG_BLOCK)[None, :]
    attention_scores = jnp.where(causal[None, None], attention_scores, 0.0)
    inner = jnp.einsum(
        "nhts,nhsv->nhtv", attention_scores, block_inputs, precision=highest_precision
    )
    contributions = jnp.einsum(
        "nhsk,nhsv->nhkv", final_keys, block_inputs, precision=highest_precision
    )
    initial = jnp.zeros((device_heads, HG_DK, HG_DV), jnp.float32)
    local_state, block_starts = lax.scan(carry_step, initial, (final_decay, contributions))
    device_decay = jnp.sum(final_decay, axis=0)
    before_blocks = jnp.cumsum(final_decay, axis=0) - final_decay
    incoming = prefix(
        (device_decay, local_state),
        "sp",
        combine_states,
        (jnp.zeros_like(device_decay), jnp.zeros_like(local_state)),
    )
    starts = block_starts + jnp.exp(before_blocks)[:, :, :, None] * incoming[1][None]
    recurrent = inner + jnp.einsum(
        "nhtk,nhkv->nhtv", query_rows_scaled, starts, precision=highest_precision
    )
    recurrent = recurrent.transpose(0, 2, 1, 3).reshape(row_total_count, device_heads, -1)
    rec_out = finish(recurrent, head_norm_gain, outgate_proj)
    values = convolved.astype(jnp.float32)
    totals = lax.psum((jnp.sum(values, axis=1), jnp.sum(values * values, axis=1)), "tp")
    conv_out = channel_norm(values, totals[0], totals[1], channel_norm_gain, channel_norm_bias)
    conv_part = lax.slice_in_dim(
        conv_out, 0, row_total_count // lax.axis_size("tp") * lax.axis_size("tp"), axis=0
    )
    return lax.psum_scatter(
        (
            jnp.dot(conv_part, conv_columns, preferred_element_type=jnp.float32)
            + jnp.dot(rec_out, rec_columns, preferred_element_type=jnp.float32)
        ).astype(jnp.bfloat16),
        "tp",
        scatter_dimension=0,
        tiled=True,
    )


MESH = pl.DeviceIdType.MESH
STRIDE = 2
NT = (((1,), (1,)), ((), ()))
TN = (((0,), (0,)), ((), ()))


def at(sp, tp):
    return {"sp": sp, "tp": tp}


def greet(peers):
    barrier = pltpu.get_barrier_semaphore()
    for peer in peers:
        pl.semaphore_signal(barrier, inc=1, device_id=peer, device_id_type=MESH)
    pl.semaphore_wait(barrier, len(peers))


def remote(src, dst, send, recv, peer):
    return pltpu.make_async_remote_copy(
        src_ref=src, dst_ref=dst, send_sem=send, recv_sem=recv, device_id=peer, device_id_type=MESH
    )


def layer_kernel(
    sizes, x_hbm, gain_ref, j_ref, taps, head_gain, floor, norm_gain, norm_bias,
    cv, cg, rv, og, qw, fw, co, ro, o_ref, p_ref, qf_ref, jump_ref, wo_ref,
    x_ref, raw, w_ref, held, weights, par_ref, ac_ref, ar_ref, q_s, k_s, d_s, r_s,
    conv_all, rec_all, sums, partial, got, mixed, load, *sems
):
    n_sp, n_tp, rows, depth, chans, members, width, block, channels = sizes
    sems, after = sems[:13], sems[13:]
    (send_z, send_x, send_y, send_c, lane, sib, send_w, recv_w, send_j, recv_j, send_q, recv_q, swap) = sems
    s, t = lax.axis_index("sp"), lax.axis_index("tp")
    n_z = n_sp // STRIDE
    z, x = s // STRIDE, s % STRIDE
    y, c = t // 2, t % 2
    x_peer = at(z * STRIDE + (1 - x), t)
    y_peer = at(s, (1 - y) * 2 + c)
    c_peer = at(s, y * 2 + (1 - c))
    total = held.shape[0]
    half = total // 2

    def sp_peer(k):
        return lax.rem(s + k, n_sp)

    def slot(dy, dx, dz, core):
        from_z = lax.rem(z - dz + n_z, n_z)
        from_x = (1 - x) if dx else x
        from_y = (1 - y) if dy else y
        start = from_y * half + ((from_z * STRIDE + from_x) * 2 + core) * rows
        return pl.ds(pl.multiple_of(start, rows), rows)

    def number(dy, dx, dz):
        return (dy * STRIDE + dx) * n_z + dz

    peers = [at(sp_peer(k), t) for k in range(1, n_sp)]
    peers += [at(s, lax.rem(t + k, n_tp)) for k in range(1, n_tp)]
    barrier = pltpu.get_barrier_semaphore()
    for peer in peers:
        pl.semaphore_signal(barrier, inc=1, device_id=peer, device_id_type=MESH)
    kinds = (cv, cg, rv, og, qw, fw)
    loads = [pltpu.make_async_copy(x_hbm, x_ref, load.at[0])] + [
        pltpu.make_async_copy(w, raw.at[i], load.at[1 + i]) for i, w in enumerate(kinds)
    ]
    cols = co.shape[1]
    swapped = wo_ref.at[:, pl.ds(pl.multiple_of(z % 2 * cols, cols), cols)]
    for i, w in enumerate((co, ro)):
        tall = w.shape[0]
        loads.append(pltpu.make_async_copy(w, swapped.at[i * tall : (i + 1) * tall, :], load.at[1 + len(kinds) + i]))
    for copy in loads:
        copy.start()
    own = slot(0, 0, 0, c)
    mine = held.at[own]
    loads[0].wait()
    features = x_ref[...].astype(jnp.float32)
    mine[...] = (
        features
        * lax.rsqrt(jnp.mean(features * features, axis=1, keepdims=True) + norm_eps)
        * gain_ref[...]
    ).astype(jnp.bfloat16)
    pl.semaphore_wait(barrier, len(peers))
    pending = []

    def launch(copy):
        copy.start()
        pending.append(copy)

    def pass_on(dy, dx, dz):
        here = held.at[slot(dy, dx, dz, c)]
        at_number = number(dy, dx, dz)
        if not dy:
            if not dx:
                launch(remote(here, here, send_x.at[dz], lane.at[number(0, 1, dz)], x_peer))
            launch(remote(here, here, send_y.at[at_number], lane.at[number(1, dx, dz)], y_peer))
        launch(remote(here, here, send_c.at[at_number], sib.at[at_number], c_peer))

    near_first = sorted(range(1, n_z), key=lambda k: min(k, n_z - k))
    for k in near_first:
        peer = at(lax.rem(z + k, n_z) * STRIDE + x, t)
        launch(remote(mine, mine, send_z.at[k], lane.at[k], peer))
    pass_on(0, 0, 0)
    for k in range(1, n_sp):
        launch(remote(j_ref, jump_ref.at[s], send_j.at[k], recv_j.at[k], at(sp_peer(k), t)))
    jump_ref[s] = j_ref[...]
    small = [taps, head_gain, floor, norm_gain, norm_bias]
    tall = sum(v.shape[0] for v in small)
    filler = jnp.zeros((-tall % 8, taps.shape[1]), jnp.float32)
    par_ref[...] = jnp.concatenate([v[...] for v in small] + [filler], axis=0).T
    for i in range(len(kinds)):
        loads[1 + i].wait()
        turned = raw[i].T
        for d in range(n_sp):
            w_ref[d, i * chans : (i + 1) * chans, :] = turned[d * chans : (d + 1) * chans]
    my_columns = pl.ds(pl.multiple_of(s * depth, depth), depth)

    def send_weights(dx, dz):
        other = lax.rem(z + dz, n_z) * STRIDE + ((1 - x) if dx else x)
        k = dx * n_z + dz
        launch(remote(w_ref.at[other], weights.at[:, my_columns], send_w.at[k], recv_w.at[k], at(other, t)))

    for dz in near_first:
        send_weights(0, dz)
    for dz in [0] + near_first:
        send_weights(1, dz)
    weights[:, my_columns] = w_ref[s]
    for copy in loads[1 + len(kinds) :]:
        copy.wait()
    partner = at((z + 1 - z % 2 * 2) * STRIDE + x, t)
    launch(remote(swapped, swapped, swap.at[0], swap.at[1], partner))

    def arrived(dy, dx, dz):
        here = held.at[slot(dy, dx, dz, c)]
        remote(here, here, send_c.at[0], lane.at[number(dy, dx, dz)], c_peer).wait_recv()
        pass_on(dy, dx, dz)

    order = []
    for dz in near_first:
        order += [(0, dz), (1, 0 if dz == near_first[0] else order[-2][1])]
    order.append((1, near_first[-1]))
    for dx, dz in order:
        arrived(0, dx, dz)
    across = [(0, 0)] + order
    early = len(across) // 2 + 1
    for dx, dz in across[:early]:
        arrived(1, dx, dz)
    for dx in range(STRIDE):
        for dz in range(n_z):
            if dx or dz:
                source = lax.rem(z - dz + n_z, n_z) * STRIDE + ((1 - x) if dx else x)
                there = weights.at[:, pl.ds(pl.multiple_of(source * depth, depth), depth)]
                k = dx * n_z + dz
                remote(there, there, send_w.at[k], recv_w.at[k], c_peer).wait_recv()
    member = lax.rem(s, members)
    first = s - member

    def project_half(dy):
        for dx in range(STRIDE):
            for dz in range(n_z):
                here = held.at[slot(dy, dx, dz, 1 - c)]
                remote(here, here, send_c.at[0], sib.at[number(dy, dx, dz)], c_peer).wait_recv()
        base = ((1 - y) if dy else y) * half
        step = min(256, half)
        for start in range(0, half, step):
            span = pl.ds(pl.multiple_of(base + start, step), step)
            piece = lax.dot_general(
                held[span, :], weights[...], NT, preferred_element_type=jnp.float32
            ).T.astype(jnp.bfloat16)
            qf_ref[member, :, span] = piece[4 * chans :]
            p_ref[:, span] = piece[: 4 * chans]
        window = pl.ds(pl.multiple_of(base, half), half)
        for k in range(1, members):
            peer = at(first + lax.rem(member + k, members), t)
            block = qf_ref.at[member, :, window]
            launch(remote(block, block, send_q.at[dy, k], recv_q.at[dy, k], peer))

    project_half(0)
    for dx, dz in across[early:]:
        arrived(1, dx, dz)
    project_half(1)
    f32, bf16 = jnp.float32, jnp.bfloat16
    own_params = par_ref[pl.ds(pl.multiple_of(s * chans, chans), chans), :]
    projected = in_order(p_ref[...].astype(f32), n_sp)
    convolve_lanes(projected, own_params, ac_ref, sizes)
    (sc_z, sc_x, rc_z, rc_x, sr_z, sr_x, rr_z, rr_x, send_s, recv_s, send_p, recv_p, send_o, recv_o) = after
    parity = z % 2

    def spread(src, dst, sz, sx, rz, rx):
        for k in near_first:
            z_to = lax.rem(z + k, n_z)
            launch(remote(src.at[z_to % 2], dst.at[s], sz.at[k], rz.at[k], at(z_to * STRIDE + x, t)))
        launch(remote(src.at[parity], dst.at[s], sx.at[0], rx.at[0], x_peer))
        dst[s] = src[parity]

    def forward(dst, sz, sx, rz, rx):
        for k in near_first:
            here = dst.at[lax.rem(z - k + n_z, n_z) * STRIDE + x]
            remote(here, here, sz.at[k], rz.at[k], x_peer).wait_recv()
            launch(remote(here, here, sx.at[k], rx.at[k], x_peer))

    def collect(dst, sx, rx):
        for k in [0] + near_first:
            here = dst.at[lax.rem(z - k + n_z, n_z) * STRIDE + (1 - x)]
            remote(here, here, sx.at[k], rx.at[k], x_peer).wait_recv()

    spread(ac_ref, conv_all, sc_z, sc_x, rc_z, rc_x)
    for dy in range(2):
        window = pl.ds(pl.multiple_of(((1 - y) if dy else y) * half, half), half)
        for k in range(1, members):
            there = qf_ref.at[lax.rem(member - k + members, members), :, window]
            remote(there, there, send_q.at[dy, k], recv_q.at[dy, k], c_peer).wait_recv()
    for k in range(1, n_sp):
        there = jump_ref.at[lax.rem(s - k + n_sp, n_sp)]
        remote(there, there, send_j.at[k], recv_j.at[k], c_peer).wait_recv()
    recur(s, projected, own_params, qf_ref, jump_ref, par_ref, ar_ref, q_s, k_s, d_s, r_s, sizes)
    spread(ar_ref, rec_all, sr_z, sr_x, rr_z, rr_x)
    forward(conv_all, sc_z, sc_x, rc_z, rc_x)
    collect(conv_all, sc_x, rc_x)
    total = ac_ref.shape[2]
    conv = conv_all[...].reshape(n_sp * chans, total).astype(f32)
    sums[t, 0:1, :] = jnp.sum(conv, axis=0, keepdims=True)
    sums[t, 1:2, :] = jnp.sum(conv * conv, axis=0, keepdims=True)

    def tp_at(k):
        return lax.rem(t + k, n_tp)

    for k in range(1, n_tp):
        launch(remote(sums.at[t], sums.at[t], send_s.at[k], recv_s.at[k], at(s, tp_at(k))))
    forward(rec_all, sr_z, sr_x, rr_z, rr_x)
    for k in range(1, n_tp):
        there = sums.at[lax.rem(t - k + n_tp, n_tp)]
        remote(there, there, send_s.at[k], recv_s.at[k], x_peer).wait_recv()
    collect(rec_all, sr_x, rr_x)
    other = wo_ref.at[:, pl.ds(pl.multiple_of((1 - z % 2) * cols, cols), cols)]
    remote(other, other, swap.at[0], swap.at[1], c_peer).wait_recv()
    both = sums[0]
    for k in range(1, n_tp):
        both = both + sums[k]
    sums[n_tp] = both
    gain = par_ref[:, width + 2 : width + 3]
    bias = par_ref[:, width + 3 : width + 4]
    span = members * chans
    heads = n_sp // members
    step = rows * n_tp
    blocks = n_sp // 2
    home = (z // 2) * STRIDE + x

    def device(place):
        return (place // STRIDE * 2 + parity) * STRIDE + place % STRIDE

    def project_block(r):
        lanes = pl.ds(pl.multiple_of(lax.rem(home + r, blocks) * step, step), step)
        mean = sums[n_tp, 0:1, lanes] / channels
        scale = lax.rsqrt(sums[n_tp, 1:2, lanes] / channels - mean * mean + layer_eps)
        values = conv_all[:, :, lanes].reshape(n_sp * chans, step).astype(f32)
        shifted = (values - mean) * scale * gain + bias
        pieces = [(shifted * jax.nn.sigmoid(shifted)).astype(bf16)]
        for h in range(heads):
            group = slice(h * members, (h + 1) * members)
            square = jnp.sum(
                rec_all[group, chans:, lanes].astype(f32), axis=(0, 1), keepdims=True
            )[0]
            ups = rec_all[group, 0:chans, lanes].reshape(span, step).astype(f32)
            pieces.append((ups * lax.rsqrt(square / span + norm_eps)).astype(bf16))
        out = lax.dot_general(
            jnp.concatenate(pieces, axis=0), wo_ref[...], TN, preferred_element_type=f32
        ).astype(bf16)
        for k in range(n_tp):
            partial[k, r] = out[k * rows : (k + 1) * rows]
        for k in range(1, n_tp):
            launch(
                remote(partial.at[tp_at(k), r], got.at[k, r], send_p.at[k, r], recv_p.at[k, r], at(s, tp_at(k)))
            )

    def window(place, p):
        column = (place // STRIDE * 2 + p) * STRIDE + place % STRIDE
        return o_ref.at[:, pl.ds(pl.multiple_of(column * cols, cols), cols)]

    def finish_block(r):
        added = partial[t, r].astype(f32)
        for k in range(1, n_tp):
            remote(got.at[k, r], got.at[k, r], send_p.at[k, r], recv_p.at[k, r], x_peer).wait_recv()
            added = added + got[k, r].astype(f32)
        mixed[r] = added.astype(bf16)
        for p in range(2):
            piece = mixed.at[r, :, p * cols : (p + 1) * cols]
            if r:
                to = at(device(lax.rem(home + r, blocks)), t)
                launch(remote(piece, window(home, p), send_o.at[r, p], recv_o.at[r, p], to))
            else:
                window(home, p)[...] = piece[...]

    sequence = list(range(1, blocks)) + [0]
    for r in sequence:
        project_block(r)
    for r in sequence:
        finish_block(r)
    for r in range(1, blocks):
        for p in range(2):
            there = window(lax.rem(home - r + blocks, blocks), p)
            remote(there, there, send_o.at[r, p], recv_o.at[r, p], x_peer).wait_recv()
    for copy in pending:
        copy.wait_send()


def in_order(array, n_sp):
    half = array.shape[1] // 2
    own = half // n_sp
    return jnp.concatenate(
        [
            array[:, side * half + b * own : side * half + (b + 1) * own]
            for b in range(n_sp)
            for side in range(2)
        ],
        axis=1,
    )


def put(ref, n_sp, start, stop, array):
    part = array.shape[1] // n_sp
    for b in range(n_sp):
        place = (b // (2 * STRIDE)) * STRIDE + b % STRIDE
        ref[(b // STRIDE) % 2, start:stop, place * part : (place + 1) * part] = array[
            :, b * part : (b + 1) * part
        ]


def convolve_lanes(projected, mine, ac_ref, sizes):
    n_sp, chans, width = sizes[0], sizes[4], sizes[6]
    value = projected[0:chans]
    gate = projected[chans : 2 * chans]
    gated = value * jax.nn.sigmoid(gate)
    place = lax.broadcasted_iota(jnp.int32, gated.shape, 1)
    conv = gated * mine[:, width - 1 : width]
    for back in range(1, width):
        moved = jnp.where(place >= back, pltpu.roll(gated, back, 1), 0.0)
        conv = conv + moved * mine[:, width - 1 - back : width - back]
    put(ac_ref, n_sp, 0, chans, conv.astype(jnp.bfloat16))


def recur(s, projected, mine, qf_ref, jump_ref, par_ref, ar_ref, q_s, k_s, d_s, r_s, sizes):
    n_sp, n_tp, rows, depth, chans, members, width, block, channels = sizes
    total = projected.shape[1]
    part = total // n_sp
    f32, bf16 = jnp.float32, jnp.bfloat16
    head = s // members
    span = chans * members
    margin = par_ref[pl.ds(pl.multiple_of(head * span, span), span), width + 1 : width + 2]
    picked = lax.broadcasted_iota(jnp.int32, jump_ref.shape[1:], 0) == head
    arranged = [in_order(qf_ref[m].astype(f32), n_sp) for m in range(members)]
    for b in range(n_sp):
        lanes = slice(b * part, (b + 1) * part)
        jump = jnp.sum(jnp.where(picked, jump_ref[b], 0.0), axis=0, keepdims=True)
        both = [arranged[m][:, lanes] for m in range(members)]
        query = jnp.concatenate([v[:chans] for v in both], axis=0)
        forget = jnp.concatenate([v[chans:] for v in both], axis=0)
        key = margin * jax.nn.sigmoid(-forget)
        q_s[lanes, :] = (query * jax.nn.sigmoid(query)).T
        k_s[lanes, :] = key.T
        d_s[lanes, :] = (jnp.log1p(-key) + jump).T
    low = lax.broadcasted_iota(jnp.int32, (block, block), 0) >= lax.broadcasted_iota(
        jnp.int32, (block, block), 1
    )
    tri = low.astype(bf16)
    inputs = projected[2 * chans : 3 * chans].T.astype(bf16)
    state = jnp.zeros((span, chans), f32)
    for n in range(total // block):
        at_rows = slice(n * block, (n + 1) * block)
        decay = d_s[at_rows, :]
        high = decay.astype(bf16)
        rest = (decay - high.astype(f32)).astype(bf16)
        cum = jnp.dot(tri, high, preferred_element_type=f32) + jnp.dot(
            tri, rest, preferred_element_type=f32
        )
        last = cum[block - 1 : block, :]
        qs = (q_s[at_rows, :] * jnp.exp(cum)).astype(bf16)
        key = k_s[at_rows, :]
        ks = (key * jnp.exp(-cum)).astype(bf16)
        kf = (key * jnp.exp(last - cum)).astype(bf16)
        rows_in = inputs[at_rows, :]
        scores = lax.dot_general(qs, ks, NT, preferred_element_type=f32)
        scores = jnp.where(low, scores, 0.0).astype(bf16)
        r_s[at_rows, :] = jnp.dot(scores, rows_in, preferred_element_type=f32) + jnp.dot(
            qs, state.astype(bf16), preferred_element_type=f32
        )
        state = jnp.exp(last).T * state + lax.dot_general(
            kf, rows_in, TN, preferred_element_type=f32
        )
    rec = r_s[...].T
    outgate = projected[3 * chans : 4 * chans]
    square = jnp.sum(rec * rec, axis=0, keepdims=True)
    put(
        ar_ref,
        n_sp,
        0,
        chans,
        (rec * mine[:, width : width + 1] * (outgate * jax.nn.sigmoid(outgate))).astype(bf16),
    )
    upper = square.astype(bf16).astype(f32)
    tall = ar_ref.shape[1]
    line = lax.broadcasted_iota(jnp.int32, (tall - chans, total), 0)
    put(
        ar_ref,
        n_sp,
        chans,
        tall,
        jnp.where(line == 0, upper, jnp.where(line == 1, square - upper, 0.0)).astype(bf16),
    )


def spread_channels(n_sp, n_tp,
    tokens,
    input_norm_gain,
    convolution_value_weight,
    convolution_gate_weight,
    depthwise_filter_taps,
    channel_norm_gain,
    channel_norm_bias,
    query_projection_weight,
    forget_gate_weight,
    recurrence_value_weight,
    output_gate_weight,
    forget_floor_margin,
    decay_jump_terms,
    head_norm_gain,
    convolution_output_weight,
    recurrence_output_weight,
):
    rows, model = tokens.shape
    total = rows * n_sp * n_tp
    depth, group_chans = convolution_value_weight.shape
    chans = group_chans // n_sp
    heads, part = decay_jump_terms.shape
    members = n_sp // heads
    width = depthwise_filter_taps.shape[0]
    kinds = (
        convolution_value_weight,
        convolution_gate_weight,
        recurrence_value_weight,
        output_gate_weight,
        query_projection_weight,
        forget_gate_weight,
    )
    cols = convolution_output_weight.shape[1]
    vmem = pl.BlockSpec(memory_space=pltpu.VMEM)
    anywhere = pl.BlockSpec(memory_space=pl.ANY)
    dma = pltpu.SemaphoreType.DMA
    bf16, f32 = jnp.bfloat16, jnp.float32
    n_z = n_sp // STRIDE
    lanes = 2 * n_sp
    span = members * chans
    blocks = n_sp // 2
    sums_rows = 16
    n_params = width + 4 + -(width + 4) % 8
    return pl.pallas_call(
        functools.partial(
            layer_kernel,
            (n_sp, n_tp, rows, depth, chans, members, width, HG_BLOCK, group_chans * n_tp),
        ),
        out_shape=jax.ShapeDtypeStruct((rows, model), bf16),
        in_specs=[anywhere] + [vmem] * 7 + [anywhere] * (len(kinds) + 2),
        out_specs=vmem,
        scratch_shapes=[
            pltpu.VMEM((4 * chans, total), bf16),
            pltpu.VMEM((members, 2 * chans, total), bf16),
            pltpu.VMEM((n_sp, *decay_jump_terms.shape), f32),
            pltpu.VMEM((2 * group_chans, 2 * cols), bf16),
            pltpu.VMEM((rows, model), bf16),
            pltpu.VMEM((len(kinds), depth, group_chans), bf16),
            pltpu.VMEM((n_sp, len(kinds) * chans, depth), bf16),
            pltpu.VMEM((total, model), bf16),
            pltpu.VMEM((len(kinds) * chans, model), bf16),
            pltpu.VMEM((group_chans, n_params), f32),
            pltpu.VMEM((2, chans, total // 2), bf16),
            pltpu.VMEM((2, chans + sums_rows, total // 2), bf16),
            pltpu.VMEM((total, span), f32),
            pltpu.VMEM((total, span), f32),
            pltpu.VMEM((total, span), f32),
            pltpu.VMEM((total, chans), f32),
            pltpu.VMEM((n_sp, chans, total // 2), bf16),
            pltpu.VMEM((n_sp, chans + sums_rows, total // 2), bf16),
            pltpu.VMEM((n_tp + 1, 8, total // 2), f32),
            pltpu.VMEM((n_tp, blocks, rows, 2 * cols), bf16),
            pltpu.VMEM((n_tp, blocks, rows, 2 * cols), bf16),
            pltpu.VMEM((blocks, rows, 2 * cols), bf16),
            dma((3 + len(kinds),)),
            dma((n_z,)),
            dma((n_z,)),
            dma((lanes,)),
            dma((lanes,)),
            dma((lanes,)),
            dma((lanes,)),
            dma((n_sp,)),
            dma((n_sp,)),
            dma((n_sp,)),
            dma((n_sp,)),
            dma((2, members)),
            dma((2, members)),
            dma((2,)),
        ]
        + [dma((n_z,))] * 8
        + [
            dma((n_tp,)),
            dma((n_tp,)),
            dma((n_tp, blocks)),
            dma((n_tp, blocks)),
            dma((blocks, 2)),
            dma((blocks, 2)),
        ],
        compiler_params=pltpu.CompilerParams(collective_id=0, has_side_effects=True),
        name="layer",
    )(
        tokens,
        input_norm_gain[None, :],
        decay_jump_terms,
        depthwise_filter_taps,
        head_norm_gain[None, :],
        forget_floor_margin[None, :],
        channel_norm_gain[None, :],
        channel_norm_bias[None, :],
        *kinds,
        convolution_output_weight,
        recurrence_output_weight,
    )


def layer(n_sp, n_tp, *arrays):
    rows, model = arrays[0].shape
    group_chans = arrays[2].shape[1]
    heads = arrays[12].shape[0]
    gathered_bytes = rows * n_sp * n_tp * model * arrays[0].dtype.itemsize
    fits = gathered_bytes <= 2**23
    even = n_tp == 4 and n_sp % heads == 0 and n_sp % (2 * STRIDE) == 0 and group_chans % (32 * n_sp) == 0
    if fits and even:
        return spread_channels(n_sp, n_tp, *arrays)
    return per_device(*arrays)


def solution(mesh):
    in_specs = (
        P(("sp", "tp"), None),
        P(),
        P("sp", "tp"),
        P("sp", "tp"),
        P(None, "tp"),
        P("tp"),
        P("tp"),
        P("sp", "tp"),
        P("sp", "tp"),
        P("sp", "tp"),
        P("sp", "tp"),
        P("tp"),
        P("tp", "sp"),
        P("tp"),
        P("tp", "sp"),
        P("tp", "sp"),
    )
    out_specs = P(("sp", "tp"), None)
    return jax.shard_map(
        functools.partial(layer, mesh.shape["sp"], mesh.shape["tp"]), mesh=mesh, in_specs=in_specs, out_specs=out_specs, check_vma=False
    )
```

```python
import functools

import jax
import jax.numpy as jnp
from jax import lax
from jax.experimental import pallas as pl
from jax.experimental.pallas import tpu as pltpu
from jax.sharding import PartitionSpec as P

CONV_CH = 1024
HG_DK = 128
HG_DV = 128
HG_BLOCK = 64


norm_eps = 1e-06
layer_eps = 1e-05
highest_precision = lax.Precision.HIGHEST


def passed_along(value, axis, steps):
    count = lax.axis_size(axis)
    initial, last = (max(0, -steps), min(count, count - steps))
    return lax.ppermute(value, axis, [(source, source + steps) for source in range(initial, last)])


def prefix(x, axis, combine, identity):
    size, mine = (lax.axis_size(axis), lax.axis_index(axis))
    everything = jax.tree.map(
        lambda part, kind: lax.all_gather(part.astype(kind), axis), x, (jnp.bfloat16, jnp.bfloat16)
    )
    start = jax.tree.map(
        lambda part, zero: jnp.broadcast_to(jnp.asarray(zero, part.dtype), part.shape), x, identity
    )

    def lap(k, before):
        reached = k < mine
        new = combine(
            before, jax.tree.map(lambda part, own: part[k].astype(own.dtype), everything, x)
        )
        return jax.tree.map(lambda a, b: jnp.where(reached, a, b), new, before)

    return lax.fori_loop(0, size, lap, start)


def convolve(gated, kernel):
    return lax.conv_general_dilated(
        gated[None],
        kernel[:, None, :],
        (1,),
        "VALID",
        dimension_numbers=("NWC", "WIO", "NWC"),
        feature_group_count=gated.shape[1],
        precision=highest_precision,
    )[0]


def channel_norm(values, first_sum, second_sum, gain, bias):
    mean_value = first_sum[:, None] / CONV_CH
    variance = second_sum[:, None] / CONV_CH - mean_value * mean_value
    shifted = (values - mean_value) * lax.rsqrt(variance + layer_eps) * gain + bias
    return jax.nn.silu(shifted).astype(jnp.bfloat16)


def gate_factors(query_projected, forget_projected, forget_floor_margin, decay_jump_rows):
    row_total_count = query_projected.shape[0]
    head_total_count = decay_jump_rows.shape[1]
    query_rows = jax.nn.silu(query_projected.astype(jnp.float32))
    log_forget_gate = jnp.logaddexp(
        jnp.log1p(-forget_floor_margin),
        jnp.log(forget_floor_margin) + jax.nn.log_sigmoid(forget_projected.astype(jnp.float32)),
    )
    key_gate_values = -jnp.expm1(log_forget_gate)
    log_decay_running = (
        log_forget_gate.reshape(row_total_count, head_total_count, -1) + decay_jump_rows[:, :, None]
    )
    return (
        query_rows.reshape(row_total_count, head_total_count, -1),
        key_gate_values.reshape(row_total_count, head_total_count, -1),
        log_decay_running,
    )


def finish(recurrent, gain, outgate_proj):
    row_total_count = recurrent.shape[0]
    scaled = recurrent * lax.rsqrt(
        jnp.mean(recurrent * recurrent, axis=2, keepdims=True) + norm_eps
    )
    gated_out = (
        scaled.reshape(row_total_count, -1) * gain * jax.nn.silu(outgate_proj.astype(jnp.float32))
    )
    return gated_out.astype(jnp.bfloat16)


def combine_states(first_part, second_part):
    return (
        first_part[0] + second_part[0],
        jnp.exp(second_part[0])[:, :, None] * first_part[1] + second_part[1],
    )


def carry_step(recurrence_state, block_parts):
    decay_end, contribution = block_parts
    return (jnp.exp(decay_end)[:, :, None] * recurrence_state + contribution, recurrence_state)


def per_device(
    tokens,
    input_norm_gain,
    convolution_value_weight,
    convolution_gate_weight,
    depthwise_filter_taps,
    channel_norm_gain,
    channel_norm_bias,
    query_projection_weight,
    forget_gate_weight,
    recurrence_value_weight,
    output_gate_weight,
    forget_floor_margin,
    decay_jump_terms,
    head_norm_gain,
    convolution_output_weight,
    recurrence_output_weight,
):
    features = tokens.astype(jnp.float32)
    normed = (
        features
        * lax.rsqrt(jnp.mean(features * features, axis=1, keepdims=True) + norm_eps)
        * input_norm_gain
    ).astype(jnp.bfloat16)
    gathered = (
        lax.all_gather(convolution_value_weight, "sp", axis=0, tiled=True),
        lax.all_gather(convolution_gate_weight, "sp", axis=0, tiled=True),
        lax.all_gather(query_projection_weight, "sp", axis=0, tiled=True),
        lax.all_gather(forget_gate_weight, "sp", axis=0, tiled=True),
        lax.all_gather(recurrence_value_weight, "sp", axis=0, tiled=True),
        lax.all_gather(output_gate_weight, "sp", axis=0, tiled=True),
        lax.all_gather(convolution_output_weight, "sp", axis=1, tiled=True),
        lax.all_gather(recurrence_output_weight, "sp", axis=1, tiled=True),
    )
    projection_weights = gathered[:6]
    conv_columns = gathered[6]
    rec_columns = gathered[7]

    def project(row_piece):
        return jnp.concatenate(
            [
                jnp.dot(row_piece, weight, preferred_element_type=jnp.float32).astype(jnp.bfloat16)
                for weight in projection_weights
            ],
            axis=1,
        )

    projected = project(lax.all_gather(normed, "tp", axis=0, tiled=True))
    offsets = []
    position = 0
    for weight in projection_weights[:-1]:
        position = position + weight.shape[1]
        offsets.append(position)
    value_proj, gate_proj, query_projected, forget_projected, input_proj, outgate_proj = jnp.split(
        projected, offsets, axis=1
    )
    row_total_count = value_proj.shape[0]
    rim_rows = depthwise_filter_taps.shape[0] - 1
    tail_value, tail_gate = passed_along(
        (value_proj[row_total_count - rim_rows :], gate_proj[row_total_count - rim_rows :]), "sp", 1
    )
    value_ext = jnp.concatenate([tail_value, value_proj], axis=0)
    gate_ext = jnp.concatenate([tail_gate, gate_proj], axis=0)
    gated = value_ext.astype(jnp.float32) * jax.nn.sigmoid(gate_ext.astype(jnp.float32))
    convolved = convolve(gated, depthwise_filter_taps).astype(jnp.bfloat16)
    device_heads = decay_jump_terms.shape[0]
    query_rows, key_gate_values, log_decay_running = gate_factors(
        query_projected, forget_projected, forget_floor_margin, decay_jump_terms.T
    )
    input_rows = input_proj.astype(jnp.float32).reshape(row_total_count, device_heads, -1)
    block_count = row_total_count // HG_BLOCK

    def to_blocks(array):
        return array.reshape(block_count, HG_BLOCK, device_heads, -1).transpose(0, 2, 1, 3)

    block_queries = to_blocks(query_rows)
    block_keys = to_blocks(key_gate_values)
    block_inputs = to_blocks(input_rows)
    cumulative = jnp.cumsum(to_blocks(log_decay_running), axis=2)
    final_decay = cumulative[:, :, -1, :]
    query_rows_scaled = block_queries * jnp.exp(cumulative)
    scaled_keys = block_keys * jnp.exp(-cumulative)
    final_keys = block_keys * jnp.exp(final_decay[:, :, None, :] - cumulative)
    attention_scores = jnp.einsum(
        "nhtk,nhsk->nhts", query_rows_scaled, scaled_keys, precision=highest_precision
    )
    causal = jnp.arange(HG_BLOCK)[:, None] >= jnp.arange(HG_BLOCK)[None, :]
    attention_scores = jnp.where(causal[None, None], attention_scores, 0.0)
    inner = jnp.einsum(
        "nhts,nhsv->nhtv", attention_scores, block_inputs, precision=highest_precision
    )
    contributions = jnp.einsum(
        "nhsk,nhsv->nhkv", final_keys, block_inputs, precision=highest_precision
    )
    initial = jnp.zeros((device_heads, HG_DK, HG_DV), jnp.float32)
    local_state, block_starts = lax.scan(carry_step, initial, (final_decay, contributions))
    device_decay = jnp.sum(final_decay, axis=0)
    before_blocks = jnp.cumsum(final_decay, axis=0) - final_decay
    incoming = prefix(
        (device_decay, local_state),
        "sp",
        combine_states,
        (jnp.zeros_like(device_decay), jnp.zeros_like(local_state)),
    )
    starts = block_starts + jnp.exp(before_blocks)[:, :, :, None] * incoming[1][None]
    recurrent = inner + jnp.einsum(
        "nhtk,nhkv->nhtv", query_rows_scaled, starts, precision=highest_precision
    )
    recurrent = recurrent.transpose(0, 2, 1, 3).reshape(row_total_count, device_heads, -1)
    rec_out = finish(recurrent, head_norm_gain, outgate_proj)
    values = convolved.astype(jnp.float32)
    totals = lax.psum((jnp.sum(values, axis=1), jnp.sum(values * values, axis=1)), "tp")
    conv_out = channel_norm(values, totals[0], totals[1], channel_norm_gain, channel_norm_bias)
    conv_part = lax.slice_in_dim(
        conv_out, 0, row_total_count // lax.axis_size("tp") * lax.axis_size("tp"), axis=0
    )
    return lax.psum_scatter(
        (
            jnp.dot(conv_part, conv_columns, preferred_element_type=jnp.float32)
            + jnp.dot(rec_out, rec_columns, preferred_element_type=jnp.float32)
        ).astype(jnp.bfloat16),
        "tp",
        scatter_dimension=0,
        tiled=True,
    )


MESH = pl.DeviceIdType.MESH
STRIDE = 2
NT = (((1,), (1,)), ((), ()))
TN = (((0,), (0,)), ((), ()))


def at(sp, tp):
    return {"sp": sp, "tp": tp}


def greet(peers):
    barrier = pltpu.get_barrier_semaphore()
    for peer in peers:
        pl.semaphore_signal(barrier, inc=1, device_id=peer, device_id_type=MESH)
    pl.semaphore_wait(barrier, len(peers))


def remote(src, dst, send, recv, peer):
    return pltpu.make_async_remote_copy(
        src_ref=src, dst_ref=dst, send_sem=send, recv_sem=recv, device_id=peer, device_id_type=MESH
    )


def layer_kernel(
    sizes, x_hbm, gain_ref, j_ref, taps, head_gain, floor, norm_gain, norm_bias,
    cv, cg, rv, og, qw, fw, co, ro, o_ref, p_ref, qf_ref, jump_ref, wo_ref,
    x_ref, raw, w_ref, held, weights, par_ref, ac_ref, ar_ref, q_s, k_s, d_s, r_s,
    conv_all, rec_all, sums, partial, got, mixed, load, *sems
):
    n_sp, n_tp, rows, depth, chans, members, width, block, channels = sizes
    sems, after = sems[:13], sems[13:]
    (send_z, send_x, send_y, send_c, lane, sib, send_w, recv_w, send_j, recv_j, send_q, recv_q, swap) = sems
    s, t = lax.axis_index("sp"), lax.axis_index("tp")
    n_z = n_sp // STRIDE
    z, x = s // STRIDE, s % STRIDE
    y, c = t // 2, t % 2
    x_peer = at(z * STRIDE + (1 - x), t)
    y_peer = at(s, (1 - y) * 2 + c)
    c_peer = at(s, y * 2 + (1 - c))
    total = held.shape[0]
    half = total // 2

    def sp_peer(k):
        return lax.rem(s + k, n_sp)

    def slot(dy, dx, dz, core):
        from_z = lax.rem(z - dz + n_z, n_z)
        from_x = (1 - x) if dx else x
        from_y = (1 - y) if dy else y
        start = from_y * half + ((from_z * STRIDE + from_x) * 2 + core) * rows
        return pl.ds(pl.multiple_of(start, rows), rows)

    def number(dy, dx, dz):
        return (dy * STRIDE + dx) * n_z + dz

    peers = [at(sp_peer(k), t) for k in range(1, n_sp)]
    peers += [at(s, lax.rem(t + k, n_tp)) for k in range(1, n_tp)]
    barrier = pltpu.get_barrier_semaphore()
    for peer in peers:
        pl.semaphore_signal(barrier, inc=1, device_id=peer, device_id_type=MESH)
    kinds = (cv, cg, rv, og, qw, fw)
    loads = [pltpu.make_async_copy(x_hbm, x_ref, load.at[0])] + [
        pltpu.make_async_copy(w, raw.at[i], load.at[1 + i]) for i, w in enumerate(kinds)
    ]
    cols = co.shape[1]
    swapped = wo_ref.at[:, pl.ds(pl.multiple_of(z % 2 * cols, cols), cols)]
    for i, w in enumerate((co, ro)):
        tall = w.shape[0]
        loads.append(pltpu.make_async_copy(w, swapped.at[i * tall : (i + 1) * tall, :], load.at[1 + len(kinds) + i]))
    for copy in loads:
        copy.start()
    own = slot(0, 0, 0, c)
    mine = held.at[own]
    loads[0].wait()
    features = x_ref[...].astype(jnp.float32)
    mine[...] = (
        features
        * lax.rsqrt(jnp.mean(features * features, axis=1, keepdims=True) + norm_eps)
        * gain_ref[...]
    ).astype(jnp.bfloat16)
    pl.semaphore_wait(barrier, len(peers))
    pending = []

    def launch(copy):
        copy.start()
        pending.append(copy)

    def pass_on(dy, dx, dz):
        here = held.at[slot(dy, dx, dz, c)]
        at_number = number(dy, dx, dz)
        if not dy:
            if not dx:
                launch(remote(here, here, send_x.at[dz], lane.at[number(0, 1, dz)], x_peer))
            if not (dx and dz == n_z - 1):
                launch(remote(here, here, send_y.at[at_number], lane.at[number(1, dx, dz)], y_peer))
        elif not dx and dz == n_z - 1:
            launch(remote(here, here, send_y.at[at_number], lane.at[number(1, 1, dz)], x_peer))
        launch(remote(here, here, send_c.at[at_number], sib.at[at_number], c_peer))

    near_first = sorted(range(1, n_z), key=lambda k: min(k, n_z - k))
    for k in near_first:
        peer = at(lax.rem(z + k, n_z) * STRIDE + x, t)
        launch(remote(mine, mine, send_z.at[k], lane.at[k], peer))
    pass_on(0, 0, 0)
    for k in range(1, n_sp):
        launch(remote(j_ref, jump_ref.at[s], send_j.at[k], recv_j.at[k], at(sp_peer(k), t)))
    jump_ref[s] = j_ref[...]
    small = [taps, head_gain, floor, norm_gain, norm_bias]
    tall = sum(v.shape[0] for v in small)
    filler = jnp.zeros((-tall % 8, taps.shape[1]), jnp.float32)
    par_ref[...] = jnp.concatenate([v[...] for v in small] + [filler], axis=0).T
    for i in range(len(kinds)):
        loads[1 + i].wait()
        turned = raw[i].T
        for d in range(n_sp):
            w_ref[d, i * chans : (i + 1) * chans, :] = turned[d * chans : (d + 1) * chans]
    my_columns = pl.ds(pl.multiple_of(s * depth, depth), depth)

    def send_weights(dx, dz):
        other = lax.rem(z + dz, n_z) * STRIDE + ((1 - x) if dx else x)
        k = dx * n_z + dz
        launch(remote(w_ref.at[other], weights.at[:, my_columns], send_w.at[k], recv_w.at[k], at(other, t)))

    for dz in near_first:
        send_weights(0, dz)
    for dz in [0] + near_first:
        send_weights(1, dz)
    weights[:, my_columns] = w_ref[s]
    for copy in loads[1 + len(kinds) :]:
        copy.wait()
    partner = at((z + 1 - z % 2 * 2) * STRIDE + x, t)
    launch(remote(swapped, swapped, swap.at[0], swap.at[1], partner))

    def arrived(dy, dx, dz):
        here = held.at[slot(dy, dx, dz, c)]
        remote(here, here, send_c.at[0], lane.at[number(dy, dx, dz)], c_peer).wait_recv()
        pass_on(dy, dx, dz)

    order = []
    for dz in near_first:
        order += [(0, dz), (1, 0 if dz == near_first[0] else order[-2][1])]
    order.append((1, near_first[-1]))
    for dx, dz in order:
        arrived(0, dx, dz)
    across = [(0, 0)] + order
    early = len(across) // 2 + 1
    for dx, dz in across[:early]:
        arrived(1, dx, dz)
    for dx in range(STRIDE):
        for dz in range(n_z):
            if dx or dz:
                source = lax.rem(z - dz + n_z, n_z) * STRIDE + ((1 - x) if dx else x)
                there = weights.at[:, pl.ds(pl.multiple_of(source * depth, depth), depth)]
                k = dx * n_z + dz
                remote(there, there, send_w.at[k], recv_w.at[k], c_peer).wait_recv()
    member = lax.rem(s, members)
    first = s - member

    def project_half(dy):
        for dx in range(STRIDE):
            for dz in range(n_z):
                here = held.at[slot(dy, dx, dz, 1 - c)]
                remote(here, here, send_c.at[0], sib.at[number(dy, dx, dz)], c_peer).wait_recv()
        base = ((1 - y) if dy else y) * half
        step = min(256, half)
        for start in range(0, half, step):
            span = pl.ds(pl.multiple_of(base + start, step), step)
            piece = lax.dot_general(
                held[span, :], weights[...], NT, preferred_element_type=jnp.float32
            ).T.astype(jnp.bfloat16)
            qf_ref[member, :, span] = piece[4 * chans :]
            p_ref[:, span] = piece[: 4 * chans]
        window = pl.ds(pl.multiple_of(base, half), half)
        for k in range(1, members):
            peer = at(first + lax.rem(member + k, members), t)
            block = qf_ref.at[member, :, window]
            launch(remote(block, block, send_q.at[dy, k], recv_q.at[dy, k], peer))

    project_half(0)
    for dx, dz in across[early:]:
        arrived(1, dx, dz)
    project_half(1)
    f32, bf16 = jnp.float32, jnp.bfloat16
    own_params = par_ref[pl.ds(pl.multiple_of(s * chans, chans), chans), :]
    projected = in_order(p_ref[...].astype(f32), n_sp)
    convolve_lanes(projected, own_params, ac_ref, sizes)
    (sc_z, sc_x, rc_z, rc_x, sr_z, sr_x, rr_z, rr_x, send_s, recv_s, send_p, recv_p, send_o, recv_o) = after
    parity = z % 2

    def spread(src, dst, sz, sx, rz, rx):
        for k in near_first:
            z_to = lax.rem(z + k, n_z)
            launch(remote(src.at[z_to % 2], dst.at[s], sz.at[k], rz.at[k], at(z_to * STRIDE + x, t)))
        launch(remote(src.at[parity], dst.at[s], sx.at[0], rx.at[0], x_peer))
        dst[s] = src[parity]

    def forward(dst, sz, sx, rz, rx):
        for k in near_first:
            here = dst.at[lax.rem(z - k + n_z, n_z) * STRIDE + x]
            remote(here, here, sz.at[k], rz.at[k], x_peer).wait_recv()
            launch(remote(here, here, sx.at[k], rx.at[k], x_peer))

    def collect(dst, sx, rx):
        for k in [0] + near_first:
            here = dst.at[lax.rem(z - k + n_z, n_z) * STRIDE + (1 - x)]
            remote(here, here, sx.at[k], rx.at[k], x_peer).wait_recv()

    spread(ac_ref, conv_all, sc_z, sc_x, rc_z, rc_x)
    for dy in range(2):
        window = pl.ds(pl.multiple_of(((1 - y) if dy else y) * half, half), half)
        for k in range(1, members):
            there = qf_ref.at[lax.rem(member - k + members, members), :, window]
            remote(there, there, send_q.at[dy, k], recv_q.at[dy, k], c_peer).wait_recv()
    for k in range(1, n_sp):
        there = jump_ref.at[lax.rem(s - k + n_sp, n_sp)]
        remote(there, there, send_j.at[k], recv_j.at[k], c_peer).wait_recv()
    recur(s, projected, own_params, qf_ref, jump_ref, par_ref, ar_ref, q_s, k_s, d_s, r_s, sizes)
    spread(ar_ref, rec_all, sr_z, sr_x, rr_z, rr_x)
    forward(conv_all, sc_z, sc_x, rc_z, rc_x)
    collect(conv_all, sc_x, rc_x)
    total = ac_ref.shape[2]
    conv = conv_all[...].reshape(n_sp * chans, total).astype(f32)
    sums[t, 0:1, :] = jnp.sum(conv, axis=0, keepdims=True)
    sums[t, 1:2, :] = jnp.sum(conv * conv, axis=0, keepdims=True)

    def tp_at(k):
        return lax.rem(t + k, n_tp)

    for k in range(1, n_tp):
        launch(remote(sums.at[t], sums.at[t], send_s.at[k], recv_s.at[k], at(s, tp_at(k))))
    forward(rec_all, sr_z, sr_x, rr_z, rr_x)
    for k in range(1, n_tp):
        there = sums.at[lax.rem(t - k + n_tp, n_tp)]
        remote(there, there, send_s.at[k], recv_s.at[k], x_peer).wait_recv()
    collect(rec_all, sr_x, rr_x)
    other = wo_ref.at[:, pl.ds(pl.multiple_of((1 - z % 2) * cols, cols), cols)]
    remote(other, other, swap.at[0], swap.at[1], c_peer).wait_recv()
    both = sums[0]
    for k in range(1, n_tp):
        both = both + sums[k]
    sums[n_tp] = both
    gain = par_ref[:, width + 2 : width + 3]
    bias = par_ref[:, width + 3 : width + 4]
    span = members * chans
    heads = n_sp // members
    step = rows * n_tp
    blocks = n_sp // 2
    home = (z // 2) * STRIDE + x

    def device(place):
        return (place // STRIDE * 2 + parity) * STRIDE + place % STRIDE

    def project_block(r):
        lanes = pl.ds(pl.multiple_of(lax.rem(home + r, blocks) * step, step), step)
        mean = sums[n_tp, 0:1, lanes] / channels
        scale = lax.rsqrt(sums[n_tp, 1:2, lanes] / channels - mean * mean + layer_eps)
        values = conv_all[:, :, lanes].reshape(n_sp * chans, step).astype(f32)
        shifted = (values - mean) * scale * gain + bias
        pieces = [(shifted * jax.nn.sigmoid(shifted)).astype(bf16)]
        for h in range(heads):
            group = slice(h * members, (h + 1) * members)
            square = jnp.sum(
                rec_all[group, chans:, lanes].astype(f32), axis=(0, 1), keepdims=True
            )[0]
            ups = rec_all[group, 0:chans, lanes].reshape(span, step).astype(f32)
            pieces.append((ups * lax.rsqrt(square / span + norm_eps)).astype(bf16))
        out = lax.dot_general(
            jnp.concatenate(pieces, axis=0), wo_ref[...], TN, preferred_element_type=f32
        ).astype(bf16)
        for k in range(n_tp):
            partial[k, r] = out[k * rows : (k + 1) * rows]
        for k in range(1, n_tp):
            launch(
                remote(partial.at[tp_at(k), r], got.at[k, r], send_p.at[k, r], recv_p.at[k, r], at(s, tp_at(k)))
            )

    def window(place, p):
        column = (place // STRIDE * 2 + p) * STRIDE + place % STRIDE
        return o_ref.at[:, pl.ds(pl.multiple_of(column * cols, cols), cols)]

    def finish_block(r):
        added = partial[t, r].astype(f32)
        for k in range(1, n_tp):
            remote(got.at[k, r], got.at[k, r], send_p.at[k, r], recv_p.at[k, r], x_peer).wait_recv()
            added = added + got[k, r].astype(f32)
        mixed[r] = added.astype(bf16)
        for p in range(2):
            piece = mixed.at[r, :, p * cols : (p + 1) * cols]
            if r:
                to = at(device(lax.rem(home + r, blocks)), t)
                launch(remote(piece, window(home, p), send_o.at[r, p], recv_o.at[r, p], to))
            else:
                window(home, p)[...] = piece[...]

    sequence = list(range(1, blocks)) + [0]
    for i, r in enumerate(sequence):
        project_block(r)
        if i >= 2:
            finish_block(sequence[i - 2])
    for r in sequence[-2:]:
        finish_block(r)
    for r in range(1, blocks):
        for p in range(2):
            there = window(lax.rem(home - r + blocks, blocks), p)
            remote(there, there, send_o.at[r, p], recv_o.at[r, p], x_peer).wait_recv()
    for copy in pending:
        copy.wait_send()


def in_order(array, n_sp):
    half = array.shape[1] // 2
    own = half // n_sp
    return jnp.concatenate(
        [
            array[:, side * half + b * own : side * half + (b + 1) * own]
            for b in range(n_sp)
            for side in range(2)
        ],
        axis=1,
    )


def put(ref, n_sp, start, stop, array):
    part = array.shape[1] // n_sp
    for b in range(n_sp):
        place = (b // (2 * STRIDE)) * STRIDE + b % STRIDE
        ref[(b // STRIDE) % 2, start:stop, place * part : (place + 1) * part] = array[
            :, b * part : (b + 1) * part
        ]


def convolve_lanes(projected, mine, ac_ref, sizes):
    n_sp, chans, width = sizes[0], sizes[4], sizes[6]
    value = projected[0:chans]
    gate = projected[chans : 2 * chans]
    gated = value * jax.nn.sigmoid(gate)
    place = lax.broadcasted_iota(jnp.int32, gated.shape, 1)
    conv = gated * mine[:, width - 1 : width]
    for back in range(1, width):
        moved = jnp.where(place >= back, pltpu.roll(gated, back, 1), 0.0)
        conv = conv + moved * mine[:, width - 1 - back : width - back]
    put(ac_ref, n_sp, 0, chans, conv.astype(jnp.bfloat16))


def recur(s, projected, mine, qf_ref, jump_ref, par_ref, ar_ref, q_s, k_s, d_s, r_s, sizes):
    n_sp, n_tp, rows, depth, chans, members, width, block, channels = sizes
    total = projected.shape[1]
    part = total // n_sp
    f32, bf16 = jnp.float32, jnp.bfloat16
    head = s // members
    span = chans * members
    margin = par_ref[pl.ds(pl.multiple_of(head * span, span), span), width + 1 : width + 2]
    picked = lax.broadcasted_iota(jnp.int32, jump_ref.shape[1:], 0) == head
    arranged = [in_order(qf_ref[m].astype(f32), n_sp) for m in range(members)]
    for b in range(n_sp):
        lanes = slice(b * part, (b + 1) * part)
        jump = jnp.sum(jnp.where(picked, jump_ref[b], 0.0), axis=0, keepdims=True)
        both = [arranged[m][:, lanes] for m in range(members)]
        query = jnp.concatenate([v[:chans] for v in both], axis=0)
        forget = jnp.concatenate([v[chans:] for v in both], axis=0)
        key = margin * jax.nn.sigmoid(-forget)
        q_s[lanes, :] = (query * jax.nn.sigmoid(query)).T
        k_s[lanes, :] = key.T
        d_s[lanes, :] = (jnp.log1p(-key) + jump).T
    low = lax.broadcasted_iota(jnp.int32, (block, block), 0) >= lax.broadcasted_iota(
        jnp.int32, (block, block), 1
    )
    tri = low.astype(bf16)
    inputs = projected[2 * chans : 3 * chans].T.astype(bf16)
    state = jnp.zeros((span, chans), f32)
    for n in range(total // block):
        at_rows = slice(n * block, (n + 1) * block)
        decay = d_s[at_rows, :]
        high = decay.astype(bf16)
        rest = (decay - high.astype(f32)).astype(bf16)
        cum = jnp.dot(tri, high, preferred_element_type=f32) + jnp.dot(
            tri, rest, preferred_element_type=f32
        )
        last = cum[block - 1 : block, :]
        qs = (q_s[at_rows, :] * jnp.exp(cum)).astype(bf16)
        key = k_s[at_rows, :]
        ks = (key * jnp.exp(-cum)).astype(bf16)
        kf = (key * jnp.exp(last - cum)).astype(bf16)
        rows_in = inputs[at_rows, :]
        scores = lax.dot_general(qs, ks, NT, preferred_element_type=f32)
        scores = jnp.where(low, scores, 0.0).astype(bf16)
        r_s[at_rows, :] = jnp.dot(scores, rows_in, preferred_element_type=f32) + jnp.dot(
            qs, state.astype(bf16), preferred_element_type=f32
        )
        state = jnp.exp(last).T * state + lax.dot_general(
            kf, rows_in, TN, preferred_element_type=f32
        )
    rec = r_s[...].T
    outgate = projected[3 * chans : 4 * chans]
    square = jnp.sum(rec * rec, axis=0, keepdims=True)
    put(
        ar_ref,
        n_sp,
        0,
        chans,
        (rec * mine[:, width : width + 1] * (outgate * jax.nn.sigmoid(outgate))).astype(bf16),
    )
    upper = square.astype(bf16).astype(f32)
    tall = ar_ref.shape[1]
    line = lax.broadcasted_iota(jnp.int32, (tall - chans, total), 0)
    put(
        ar_ref,
        n_sp,
        chans,
        tall,
        jnp.where(line == 0, upper, jnp.where(line == 1, square - upper, 0.0)).astype(bf16),
    )


def spread_channels(n_sp, n_tp,
    tokens,
    input_norm_gain,
    convolution_value_weight,
    convolution_gate_weight,
    depthwise_filter_taps,
    channel_norm_gain,
    channel_norm_bias,
    query_projection_weight,
    forget_gate_weight,
    recurrence_value_weight,
    output_gate_weight,
    forget_floor_margin,
    decay_jump_terms,
    head_norm_gain,
    convolution_output_weight,
    recurrence_output_weight,
):
    rows, model = tokens.shape
    total = rows * n_sp * n_tp
    depth, group_chans = convolution_value_weight.shape
    chans = group_chans // n_sp
    heads, part = decay_jump_terms.shape
    members = n_sp // heads
    width = depthwise_filter_taps.shape[0]
    kinds = (
        convolution_value_weight,
        convolution_gate_weight,
        recurrence_value_weight,
        output_gate_weight,
        query_projection_weight,
        forget_gate_weight,
    )
    cols = convolution_output_weight.shape[1]
    vmem = pl.BlockSpec(memory_space=pltpu.VMEM)
    anywhere = pl.BlockSpec(memory_space=pl.ANY)
    dma = pltpu.SemaphoreType.DMA
    bf16, f32 = jnp.bfloat16, jnp.float32
    n_z = n_sp // STRIDE
    lanes = 2 * n_sp
    span = members * chans
    blocks = n_sp // 2
    sums_rows = 16
    n_params = width + 4 + -(width + 4) % 8
    return pl.pallas_call(
        functools.partial(
            layer_kernel,
            (n_sp, n_tp, rows, depth, chans, members, width, HG_BLOCK, group_chans * n_tp),
        ),
        out_shape=jax.ShapeDtypeStruct((rows, model), bf16),
        in_specs=[anywhere] + [vmem] * 7 + [anywhere] * (len(kinds) + 2),
        out_specs=vmem,
        scratch_shapes=[
            pltpu.VMEM((4 * chans, total), bf16),
            pltpu.VMEM((members, 2 * chans, total), bf16),
            pltpu.VMEM((n_sp, *decay_jump_terms.shape), f32),
            pltpu.VMEM((2 * group_chans, 2 * cols), bf16),
            pltpu.VMEM((rows, model), bf16),
            pltpu.VMEM((len(kinds), depth, group_chans), bf16),
            pltpu.VMEM((n_sp, len(kinds) * chans, depth), bf16),
            pltpu.VMEM((total, model), bf16),
            pltpu.VMEM((len(kinds) * chans, model), bf16),
            pltpu.VMEM((group_chans, n_params), f32),
            pltpu.VMEM((2, chans, total // 2), bf16),
            pltpu.VMEM((2, chans + sums_rows, total // 2), bf16),
            pltpu.VMEM((total, span), f32),
            pltpu.VMEM((total, span), f32),
            pltpu.VMEM((total, span), f32),
            pltpu.VMEM((total, chans), f32),
            pltpu.VMEM((n_sp, chans, total // 2), bf16),
            pltpu.VMEM((n_sp, chans + sums_rows, total // 2), bf16),
            pltpu.VMEM((n_tp + 1, 8, total // 2), f32),
            pltpu.VMEM((n_tp, blocks, rows, 2 * cols), bf16),
            pltpu.VMEM((n_tp, blocks, rows, 2 * cols), bf16),
            pltpu.VMEM((blocks, rows, 2 * cols), bf16),
            dma((3 + len(kinds),)),
            dma((n_z,)),
            dma((n_z,)),
            dma((lanes,)),
            dma((lanes,)),
            dma((lanes,)),
            dma((lanes,)),
            dma((n_sp,)),
            dma((n_sp,)),
            dma((n_sp,)),
            dma((n_sp,)),
            dma((2, members)),
            dma((2, members)),
            dma((2,)),
        ]
        + [dma((n_z,))] * 8
        + [
            dma((n_tp,)),
            dma((n_tp,)),
            dma((n_tp, blocks)),
            dma((n_tp, blocks)),
            dma((blocks, 2)),
            dma((blocks, 2)),
        ],
        compiler_params=pltpu.CompilerParams(collective_id=0, has_side_effects=True),
        name="layer",
    )(
        tokens,
        input_norm_gain[None, :],
        decay_jump_terms,
        depthwise_filter_taps,
        head_norm_gain[None, :],
        forget_floor_margin[None, :],
        channel_norm_gain[None, :],
        channel_norm_bias[None, :],
        *kinds,
        convolution_output_weight,
        recurrence_output_weight,
    )


def layer(n_sp, n_tp, *arrays):
    rows, model = arrays[0].shape
    group_chans = arrays[2].shape[1]
    heads = arrays[12].shape[0]
    gathered_bytes = rows * n_sp * n_tp * model * arrays[0].dtype.itemsize
    fits = gathered_bytes <= 2**23
    even = n_tp == 4 and n_sp % heads == 0 and n_sp % (2 * STRIDE) == 0 and group_chans % (32 * n_sp) == 0
    if fits and even:
        return spread_channels(n_sp, n_tp, *arrays)
    return per_device(*arrays)


def solution(mesh):
    in_specs = (
        P(("sp", "tp"), None),
        P(),
        P("sp", "tp"),
        P("sp", "tp"),
        P(None, "tp"),
        P("tp"),
        P("tp"),
        P("sp", "tp"),
        P("sp", "tp"),
        P("sp", "tp"),
        P("sp", "tp"),
        P("tp"),
        P("tp", "sp"),
        P("tp"),
        P("tp", "sp"),
        P("tp", "sp"),
    )
    out_specs = P(("sp", "tp"), None)
    return jax.shard_map(
        functools.partial(layer, mesh.shape["sp"], mesh.shape["tp"]), mesh=mesh, in_specs=in_specs, out_specs=out_specs, check_vma=False
    )
```
